32 devices in a mesh: ep: 8 (over z, x), tp: 4 (over y, core).
Axes of the slice: x: 2, y: 2, z: 4, core: 2. Of those that a mesh axis runs over, the one named last changes fastest.
Arguments:
- tokens: bfloat16 [1024, 2048], P('ep', 'tp'), may hold values from -20 to 20
- routing: int32 [1024, 2], P('ep'), may hold values from 0 to 7, all different within a row; in each aligned block of 128 rows (0 to 127, 128 to 255, ...) at most 48 rows name the same one
- gate_weights: bfloat16 [1024, 2], P('ep'), may hold values from 0 to 1, as said below
- cotangent: bfloat16 [1024, 2048], P('ep', 'tp'), may hold values from -3 to 3
- expert_gate: bfloat16 [8, 2048, 3072], P('ep', None, 'tp'), may hold values from -3 to 3
- expert_up: bfloat16 [8, 2048, 3072], P('ep', None, 'tp'), may hold values from -3 to 3
- expert_down: bfloat16 [8, 3072, 2048], P('ep', 'tp'), may hold values from -0.109375 to 0.109375
- router: bfloat16 [2048, 8], replicated, may hold values from -0.125 to 0.125
Outputs:
- token_grad: float32 [1024, 2048], P('ep', 'tp')
- gate_grad: float32 [1024, 2], P('ep')
- gate_proj_grad: bfloat16 [8, 2048, 3072], P('ep', None, 'tp')
- up_proj_grad: bfloat16 [8, 2048, 3072], P('ep', None, 'tp')
- down_proj_grad: bfloat16 [8, 3072, 2048], P('ep', 'tp')
- router_grad: float32 [8, 2048], P('ep', 'tp')
- gate_row_square: float32 [8, 2048], P('ep')
- up_row_square: float32 [8, 2048], P('ep')
- down_row_square: float32 [8, 3072], P('ep', 'tp')
The draws below stay inside these ranges and needn't reach their ends.
Inputs may be any that keep to these rules, and one draw needn't show every extreme that they name: `routing`: each token names 2 different experts. Among the 128 rows of one device no expert is named more than 48 times; some device reaches 48. `gate_weights`: each row is positive and sums to one up to rounding.
All inputs are finite; a program needn't handle non-finite values.
Results may differ from the reference program's by a relative error of at most 0.015.
Values may be sent and summed in bfloat16 or wider, within the bound.
A program may use at most 64 MiB of HBM per device.

```python
import math
import jax
import jax.numpy as jnp
import numpy as np
from jax import lax

D = 2048
FF = 3072
TOP = 2
TOK_DEV = 128
EXPERTS = 8
CAP = 48
TOKENS = 1024
N_EP = 8
N_TP = 4


def feature_scale(key, length, spread):
    place = jnp.arange(length, dtype=jnp.float32) / length
    jitter = jax.random.uniform(key, (length,), jnp.float32, -0.5, 0.5)
    return jnp.exp(jnp.log(spread) * (place - 0.5) + jitter)


def base_values(key, shape):
    return jnp.clip(jax.random.normal(key, shape, jnp.float32), -5.0, 5.0)


def scaled_matrix(key):
    values = base_values(jax.random.fold_in(key, 21), (EXPERTS, D, FF))
    spread = 3.0
    columns = feature_scale(jax.random.fold_in(key, 22), FF, spread)
    return (values * columns * D ** (-0.5)).astype(jnp.bfloat16)


def draw_tokens(key, part):
    values = base_values(jax.random.fold_in(key, 11), (TOKENS, D))
    columns = feature_scale(jax.random.fold_in(key, 12), D, 3.0)
    return (values * columns).astype(jnp.bfloat16)


def draw_gate_weights(key, part):
    logits = jax.random.uniform(key, (TOKENS, TOP), jnp.float32, -1.5, 1.5)
    return jax.nn.softmax(logits, axis=-1).astype(jnp.bfloat16)


def draw_expert_gate(key, part):
    return scaled_matrix(jax.random.fold_in(key, 31))


def draw_expert_up(key, part):
    return scaled_matrix(jax.random.fold_in(key, 32))


def shard_levels(stream_key, shape, split, least, largest):
    level = 1.0
    for dim, parts in split:
        draws = jax.random.uniform(jax.random.fold_in(jax.random.fold_in(stream_key, 6), dim), (parts,), jnp.float32, least / len(split), largest / len(split))
        level = level * jnp.repeat(jnp.exp(draws), shape[dim] // parts).reshape((-1,) + (1,) * (len(shape) - 1 - dim))
    return level


def assign_block(own_key, own, number, rows, count, top, reach, slope):
    order = jax.random.permutation(own_key, count)
    crowded, common = load_shares(count, rows * top, reach, slope, True), load_shares(count, rows * top, reach, slope, False)
    places = jnp.arange(count)

    def named(lengths, rotation):
        used = int((lengths > 0).sum())
        fixed = max(1, used // 4)
        moved = fixed + (places - fixed + rotation * (used - fixed)) % max(1, count - fixed)
        return jnp.zeros((count,), jnp.int32).at[order[jnp.where(places < fixed, places, moved)]].set(jnp.asarray(lengths, jnp.int32))

    lengths = jnp.where(number % 4 == 0, named(crowded, number // 4), named(common, number - number // 4 - 1))
    mixed = jax.random.permutation(jax.random.fold_in(own, 3), count)
    giver, sink = mixed[0:count // 2 * 2:2], mixed[1:count // 2 * 2:2]
    slack = jnp.minimum(lengths[giver] - 1, reach - lengths[sink]) // 2
    slack = jnp.where((giver == order[0]) | (sink == order[0]) | (lengths[sink] == 0), 0, jnp.maximum(slack, 0))
    moved = jax.random.randint(jax.random.fold_in(own, 4), (count // 2,), 0, 1 << 20) % (slack + 1)
    lengths = lengths.at[giver].add(-moved).at[sink].add(moved)
    items = jnp.searchsorted(jnp.cumsum(lengths), jnp.arange(rows * top), side="right").astype(jnp.int32)
    listing = items.reshape(top, rows).T
    listing = listing[jax.random.permutation(jax.random.fold_in(own, 1), rows)]
    rotation = jax.random.randint(jax.random.fold_in(own, 2), (rows, 1), 0, top)
    return jnp.take_along_axis(listing, (jnp.arange(top)[None, :] + rotation) % top, axis=1)


def load_shares(count, total, reach, slope, full):
    loads = [(1 << 20) // math.isqrt(grade ** slope) + 1 for grade in range(1, count + 1)]
    largest = reach if full else min(reach, max(-(-total // count), total * loads[0] // sum(loads)))
    least = 1 if total - largest >= count - 1 else 0
    counts, rest = [largest] + [least] * (count - 1), total - largest - least * (count - 1)
    while rest > 0:
        free = [i for i in range(1, count) if counts[i] < largest] or [i for i in range(1, count) if counts[i] < reach]
        whole, left = sum([loads[i] for i in free]), rest
        for i in free:
            more = min(reach - counts[i], max(1, left * loads[i] // whole), rest)
            counts[i] = counts[i] + more
            rest = rest - more
    return np.array(counts)


def bell_draw(stream_key, dims, scale, most, pieces=(), held_as=jnp.bfloat16):
    result = scale * jax.random.normal(stream_key, dims, jnp.float32)
    if pieces:
        result = result * shard_levels(stream_key, dims, pieces, -0.22, 0.18)
    return jnp.clip(result, -most, most).astype(held_as)


def setup_inputs(seed: int = 0) -> dict:
    arg_keys = jax.random.split(jax.random.key(seed), 9)
    tokens = draw_tokens(jax.random.fold_in(arg_keys[8], 71), 0)
    routing_keys = jax.random.split(jax.random.fold_in(arg_keys[1], 1), TOKENS // TOK_DEV)
    routing_turns = jax.random.permutation(jax.random.fold_in(arg_keys[1], 3), TOKENS // TOK_DEV)
    routing = jax.vmap(lambda own, number: assign_block(jax.random.fold_in(arg_keys[1], 2), own, number, TOK_DEV, EXPERTS, TOP, CAP, 1))(routing_keys, routing_turns).reshape((TOKENS, TOP))
    gate_weights = draw_gate_weights(jax.random.fold_in(arg_keys[8], 71), 0)
    cotangent = bell_draw(arg_keys[3], (TOKENS, D), 0.5, 3.0, ((0, 8), (1, 4)))
    expert_gate = draw_expert_gate(jax.random.fold_in(arg_keys[8], 71), 0)
    expert_up = draw_expert_up(jax.random.fold_in(arg_keys[8], 71), 0)
    expert_down = bell_draw(arg_keys[6], (EXPERTS, FF, D), FF ** -0.5, 0.109375, ((0, 8), (1, 4)))
    router = bell_draw(arg_keys[7], (D, EXPERTS), D ** -0.5, 0.125)
    return {"tokens": tokens, "routing": routing, "gate_weights": gate_weights, "cotangent": cotangent, "expert_gate": expert_gate, "expert_up": expert_up, "expert_down": expert_down, "router": router}


def reference(tokens, routing, gate_weights, cotangent, expert_gate, expert_up, expert_down, router):
    pair_count = TOK_DEV * TOP
    block_routes = routing.reshape(N_EP, pair_count)
    slot_ids = jnp.arange(CAP, dtype=jnp.int32)
    pair_ids = jnp.arange(pair_count, dtype=jnp.int32)
    block_base = (jnp.arange(N_EP, dtype=jnp.int32) * TOK_DEV)[:, None]
    hidden_local = FF // N_TP

    def one_expert(expert_index):
        hit_mask = (block_routes == expert_index).astype(jnp.int32)
        ranking = (jnp.cumsum(hit_mask, axis=1) - 1).astype(jnp.int32)
        chosen = hit_mask[:, None, :] * (ranking[:, None, :] == slot_ids[None, :, None]).astype(jnp.int32)
        source_pair = jnp.sum(chosen * pair_ids[None, None, :], axis=2).astype(jnp.int32)
        filled = jnp.sum(chosen, axis=2) > 0
        row_index = (block_base + source_pair // TOP).reshape(-1).astype(jnp.int32)
        which_slot = (source_pair % TOP).reshape(-1).astype(jnp.int32)
        live_slot = filled.reshape(-1)
        input_slots = jnp.where(live_slot[:, None], tokens[row_index], jnp.zeros((), jnp.bfloat16))
        tangent_slots = jnp.where(live_slot[:, None], cotangent[row_index], jnp.zeros((), jnp.bfloat16))
        slot_weight = jnp.where(live_slot, gate_weights[row_index, which_slot].astype(jnp.float32), jnp.float32(0.0))
        gate_matrix = expert_gate[expert_index]
        up_matrix = expert_up[expert_index]
        down_matrix = expert_down[expert_index]
        pre_gate = jnp.dot(input_slots, gate_matrix, preferred_element_type=jnp.float32)
        pre_up = jnp.dot(input_slots, up_matrix, preferred_element_type=jnp.float32)
        back_proj = jnp.dot(tangent_slots, down_matrix.T, preferred_element_type=jnp.float32)
        sigmoid_gate = jax.nn.sigmoid(pre_gate)
        active = pre_gate * sigmoid_gate
        hidden = active * pre_up
        slot_gate = jnp.sum(hidden * back_proj, axis=1)
        weight_col = slot_weight[:, None]
        scaled = (weight_col * hidden).astype(jnp.bfloat16)
        hidden_grad = weight_col * back_proj
        gate_pre_grad = (hidden_grad * pre_up * sigmoid_gate * (1.0 + pre_gate * (1.0 - sigmoid_gate))).astype(jnp.bfloat16)
        up_pre_grad = (hidden_grad * active).astype(jnp.bfloat16)
        gate_sum = jnp.dot(input_slots.T, gate_pre_grad, preferred_element_type=jnp.float32)
        up_sum = jnp.dot(input_slots.T, up_pre_grad, preferred_element_type=jnp.float32)
        down_sum = jnp.dot(scaled.T, tangent_slots, preferred_element_type=jnp.float32)
        slot_total = N_EP * CAP
        block_parts = jnp.einsum('snf,dnf->nsd',
                                 gate_pre_grad.astype(jnp.float32).reshape(slot_total, N_TP, hidden_local),
                                 gate_matrix.astype(jnp.float32).reshape(D, N_TP, hidden_local))
        block_parts = block_parts + jnp.einsum('snf,dnf->nsd',
                                               up_pre_grad.astype(jnp.float32).reshape(slot_total, N_TP, hidden_local),
                                               up_matrix.astype(jnp.float32).reshape(D, N_TP, hidden_local))
        rounded = lax.optimization_barrier(block_parts.astype(jnp.bfloat16))
        slot_token = jnp.sum(rounded.astype(jnp.float32), axis=0)
        return (slot_token.reshape(N_EP, CAP, D), slot_gate.reshape(N_EP, CAP),
                gate_sum.astype(jnp.bfloat16), up_sum.astype(jnp.bfloat16), down_sum.astype(jnp.bfloat16),
                jnp.mean(gate_sum * gate_sum, axis=1), jnp.mean(up_sum * up_sum, axis=1),
                jnp.mean(down_sum * down_sum, axis=1))

    results = lax.map(one_expert, jnp.arange(EXPERTS, dtype=jnp.int32))
    slot_token, slot_gate, gate_grads, up_grads, down_grads, gate_square, up_square, down_square = results
    labels = jnp.arange(EXPERTS, dtype=jnp.int32)
    one_hot = (block_routes[:, :, None] == labels[None, None, :]).astype(jnp.int32)
    ranking = (jnp.cumsum(one_hot, axis=1) - 1).astype(jnp.int32)
    position = jnp.sum(one_hot * ranking, axis=2).astype(jnp.int32)
    source_ids = jnp.broadcast_to(jnp.arange(N_EP, dtype=jnp.int32)[:, None], (N_EP, pair_count))
    pair_token = slot_token[block_routes, source_ids, position]
    token_part = jnp.sum(pair_token.reshape(TOKENS, TOP, D), axis=1)
    gate_grad = slot_gate[block_routes, source_ids, position].reshape(TOKENS, TOP)
    weights_f = gate_weights.astype(jnp.float32)
    mixed_term = jnp.sum(weights_f * gate_grad, axis=1, keepdims=True)
    logit_grad = weights_f * (gate_grad - mixed_term)
    signal = jnp.sum(jnp.where(routing[:, :, None] == labels[None, None, :], logit_grad[:, :, None], jnp.float32(0.0)), axis=1).astype(jnp.bfloat16)
    router_grad = jnp.dot(signal.T, tokens, preferred_element_type=jnp.float32)
    token_grad = token_part + jnp.dot(signal, router.T, preferred_element_type=jnp.float32)
    return (token_grad, gate_grad, gate_grads, up_grads, down_grads, router_grad, gate_square, up_square, down_square)
```

```python
import functools

import jax
import jax.numpy as jnp
from jax import lax
from jax.experimental import pallas as pl
from jax.experimental.pallas import tpu as pltpu
from jax.sharding import PartitionSpec as P

MESH = pl.DeviceIdType.MESH
F32 = jnp.float32
BF16 = jnp.bfloat16
VMEM = pltpu.VMEM


def matmul_nn(left_side, right_side):
    return jnp.dot(left_side, right_side, preferred_element_type=F32)


def matmul_tn(left_side, right_side):
    return lax.dot_general(
        left_side, right_side, (((0,), (0,)), ((), ())), preferred_element_type=F32
    )


def matmul_nt(left_side, right_side):
    return lax.dot_general(
        left_side, right_side, (((1,), (1,)), ((), ())), preferred_element_type=F32
    )


def loop(lower, upper, body):
    if upper - lower <= 8:
        for i in range(lower, upper):
            body(i)
    else:
        lax.fori_loop(lower, upper, lambda i, carry: (body(i), carry)[1], 0)


def place():
    ep, tp = lax.axis_index("ep"), lax.axis_index("tp")
    return ep, tp, lax.div(tp, 2), lax.rem(tp, 2)


def paired(value, step, count):
    if count & (count - 1):
        return lax.rem(value + step, count)
    out, bit = value, 1
    while bit < count:
        asked = lax.rem(lax.div(jnp.int32(step), bit), 2)
        out = out + asked * bit * (1 - 2 * lax.rem(lax.div(value, bit), 2))
        bit *= 2
    return out


def greet(n_ep, n_tp, between=None):
    ep, tp, _, _ = place()
    barrier = pltpu.get_barrier_semaphore()

    def to_ep(r):
        pl.semaphore_signal(
            barrier, inc=1, device_id=(lax.rem(ep + r, n_ep), tp), device_id_type=MESH
        )

    def to_tp(r):
        pl.semaphore_signal(
            barrier, inc=1, device_id=(ep, lax.rem(tp + r, n_tp)), device_id_type=MESH
        )

    loop(1, n_ep, to_ep)
    loop(1, n_tp, to_tp)
    if between is not None:
        between()
    pl.semaphore_wait(barrier, n_ep - 1 + n_tp - 1)


def lane_pick(n_ep, cap):
    shape = (n_ep, cap, 128)
    pick = lax.broadcasted_iota(jnp.int32, shape, 1) == lax.broadcasted_iota(jnp.int32, shape, 2)
    return pick.astype(F32).reshape(n_ep * cap, 128)


def own_block(n_ep, cap):
    shape = (n_ep, n_ep * cap)
    first = lax.broadcasted_iota(jnp.int32, shape, 0) * cap
    slot = lax.broadcasted_iota(jnp.int32, shape, 1)
    return ((slot >= first) & (slot < first + cap)).astype(F32)


def fill_slots(cap, routes_ref, weights_ref, tokens_ref, cotangent_ref, table_ref, out_ref, w_ref):
    n_ep = w_ref.shape[0]
    width = out_ref.shape[2]
    top, tok = routes_ref.shape
    routes = routes_ref[...]
    weights = weights_ref[...].astype(F32)
    labels = lax.broadcasted_iota(jnp.int32, (n_ep, tok), 0)
    hit = jnp.zeros((n_ep, tok), F32)
    chosen = jnp.zeros((n_ep, tok), F32)
    for k in range(top):
        same = routes[k : k + 1, :] == labels
        hit = hit + same.astype(F32)
        chosen = chosen + jnp.where(same, weights[k : k + 1, :], 0.0)
    square = (tok, tok)
    before = lax.broadcasted_iota(jnp.int32, square, 0) < lax.broadcasted_iota(jnp.int32, square, 1)
    count = matmul_nn(hit.astype(BF16), before.astype(F32).astype(BF16))
    position = jnp.where(hit > 0.0, count, -1.0)
    slot = lax.broadcasted_iota(jnp.int32, (n_ep, cap, tok), 1).astype(F32)
    table = (slot == position[:, None, :]).astype(F32).reshape(n_ep * cap, tok).astype(BF16)
    table_ref[...] = table
    for which, source in enumerate((tokens_ref, cotangent_ref)):
        out_ref[which] = matmul_nn(table, source[...]).astype(BF16)
    spread = matmul_nt(chosen.astype(BF16), table) * own_block(n_ep, cap)
    values = matmul_nn(spread.astype(BF16), lane_pick(n_ep, cap).astype(BF16))
    w_ref[...] = jnp.broadcast_to(values[:, None, :], w_ref.shape)


def layer_kernel(
    n_ep,
    n_tp,
    chunks,
    cap,
    routes_ref,
    weights_ref,
    tokens_ref,
    cotangent_ref,
    router_ref,
    gate_hbm,
    up_hbm,
    down_hbm,
    token_out,
    gate_out,
    term_out,
    square_out,
    down_square_out,
    gate_res,
    up_res,
    down_res,
    gate_w,
    up_w,
    down_w,
    table_ref,
    slots_ref,
    w_ref,
    full_ref,
    full_w_ref,
    pre_gate,
    pre_up,
    back_proj,
    slot_w,
    slot_sum,
    scaled_ref,
    gate_pre,
    up_pre,
    part_ref,
    gate_send_ref,
    gate_buf,
    gate_back_out,
    gate_back,
    core_buf,
    y_out,
    y_buf,
    ep_out,
    back_ref,
    square_buf,
    term_ref,
    term_buf,
    load_sem,
    own_sem,
    ep_send,
    ep_recv,
    w_send,
    w_recv,
    y_send,
    y_recv,
    core_send,
    core_recv,
    rcore_send,
    rcore_recv,
    ry_send,
    ry_recv,
    rep_send,
    rep_recv,
    tp_send,
    tp_recv,
    gate_sem_send,
    gate_sem_recv,
    sq_send,
    sq_recv,
    term_send,
    term_recv,
):
    ep, tp, y, core = place()
    n_y = n_tp // 2
    partner = y * 2 + 1 - core
    slots, features = part_ref.shape
    width = features // n_tp
    hidden = gate_w.shape[1]
    top, tok = routes_ref.shape
    per = n_ep // chunks
    rows = per * cap
    size = 2 if chunks % 2 == 0 else 1
    groups = chunks // size
    group_rows = size * rows
    exact_rows = 16 if group_rows % 16 == 0 else 8

    def cols(which):
        return pl.ds(pl.multiple_of(which * width, width), width)

    def chunk_rows(chunk):
        return pl.ds(pl.multiple_of(chunk * rows, rows), rows)

    def source_rows(source):
        return pl.ds(pl.multiple_of(source * cap, cap), cap)

    def remote(src, dst, send, recv, device):
        return pltpu.make_async_remote_copy(
            src_ref=src,
            dst_ref=dst,
            send_sem=send,
            recv_sem=recv,
            device_id=device,
            device_id_type=MESH,
        )

    def group_at(j):
        return paired(lax.div(ep, per * size), j, groups)

    def chunk_at(j, i):
        return group_at(j) * size + (i if size == 1 else lax.rem(lax.div(ep, per) + i, size))

    def ep_copy(dst, src):
        return remote(
            slots_ref.at[:, source_rows(dst), :],
            full_ref.at[:, source_rows(src), cols(tp)],
            ep_send.at[dst],
            ep_recv.at[src],
            (dst, tp),
        )

    def w_copy(dst, src):
        return remote(w_ref.at[dst], full_w_ref.at[src], w_send.at[dst], w_recv.at[src], (dst, tp))

    def y_copy(source_y, target_y, chunk):
        piece = full_ref.at[:, chunk_rows(chunk), cols(source_y * 2 + core)]
        return remote(
            piece,
            piece,
            y_send.at[target_y, chunk],
            y_recv.at[source_y, chunk],
            (ep, target_y * 2 + core),
        )

    def core_copy(source_y, source_core, chunk):
        piece = full_ref.at[:, chunk_rows(chunk), cols(source_y * 2 + source_core)]
        return remote(
            piece, piece, core_send.at[source_y, chunk], core_recv.at[source_y, chunk], (ep, partner)
        )

    def rcore_copy(target_y, chunk):
        return remote(
            part_ref.at[chunk_rows(chunk), cols(target_y * 2 + 1 - core)],
            core_buf.at[target_y, chunk_rows(chunk)],
            rcore_send.at[target_y, chunk],
            rcore_recv.at[target_y, chunk],
            (ep, partner),
        )

    def ry_copy(source_y, target_y, chunk):
        return remote(
            y_out.at[target_y, chunk_rows(chunk)],
            y_buf.at[source_y, chunk_rows(chunk)],
            ry_send.at[target_y, chunk],
            ry_recv.at[source_y, chunk],
            (ep, target_y * 2 + core),
        )

    def rep_copy(dst, src):
        return remote(
            ep_out.at[source_rows(dst)],
            back_ref.at[source_rows(src)],
            rep_send.at[dst],
            rep_recv.at[src],
            (dst, tp),
        )

    def tp_copy(dst, src):
        return remote(gate_send_ref, gate_buf.at[src], tp_send.at[dst], tp_recv.at[src], (ep, dst))

    def gate_copy(dst, src):
        return remote(
            gate_back_out.at[dst],
            gate_back.at[src],
            gate_sem_send.at[dst],
            gate_sem_recv.at[src],
            (dst, tp),
        )

    def square_copy(dst, src):
        return remote(
            square_buf.at[src], square_buf.at[src], sq_send.at[dst], sq_recv.at[src], (ep, dst)
        )

    def term_copy(dst, src):
        return remote(
            term_ref.at[dst], term_buf.at[src], term_send.at[dst], term_recv.at[src], (dst, tp)
        )

    loads = [
        pltpu.make_async_copy(hbm.at[0], vmem, load_sem.at[i])
        for i, (hbm, vmem) in enumerate(((gate_hbm, gate_w), (up_hbm, up_w), (down_hbm, down_w)))
    ]
    for load in loads:
        load.start()
    fill = functools.partial(
        fill_slots,
        cap,
        routes_ref,
        weights_ref,
        tokens_ref,
        cotangent_ref,
        table_ref,
        slots_ref,
        w_ref,
    )
    greet(n_ep, n_tp, fill)

    own_rows = pltpu.make_async_copy(
        slots_ref.at[:, source_rows(ep), :],
        full_ref.at[:, source_rows(ep), cols(tp)],
        own_sem.at[0],
    )
    own_w = pltpu.make_async_copy(w_ref.at[ep], full_w_ref.at[ep], own_sem.at[1])
    own_rows.start()
    own_w.start()

    def each_source(j, i, body):
        chunk = chunk_at(j, i)

        def one(n):
            source = chunk * per + n

            @pl.when(source != ep)
            def _():
                body(source)

        loop(0, per, one)

    def send_group(j):
        for i in range(size):
            each_source(j, i, lambda dst: ep_copy(dst, ep).start())

    loop(0, groups, send_group)

    def send_w_group(j):
        for i in range(size):
            each_source(j, i, lambda dst: w_copy(dst, ep).start())

    loop(0, groups, send_w_group)
    gate_send_ref[...] = jnp.zeros_like(gate_send_ref)
    own_rows.wait()
    own_w.wait()

    def relay(j):
        for i in range(size):
            chunk = chunk_at(j, i)
            each_source(j, i, lambda source: ep_copy(ep, source).wait_recv())
            for r in range(1, n_y):
                y_copy(y, lax.rem(y + r, n_y), chunk).start()
            core_copy(y, core, chunk).start()

    def forward(j):
        for i in range(size):
            chunk = chunk_at(j, i)
            for r in range(1, n_y):
                source_y = lax.rem(y + n_y - r, n_y)
                y_copy(source_y, y, chunk).wait_recv()
                core_copy(source_y, core, chunk).start()

    def arrive(j):
        for i in range(size):
            chunk = chunk_at(j, i)
            for r in range(n_y):
                core_copy(r, 1 - core, chunk).wait_recv()
            each_source(j, i, lambda source: w_copy(ep, source).wait_recv())

    def compute(j):
        group = group_at(j)
        at = pl.ds(pl.multiple_of(group * group_rows, group_rows), group_rows)
        first = group * (size * per)
        for n in range(size * per):
            weight = jnp.broadcast_to(full_w_ref[first + n][0:1, :], (128, 128)).T
            slot_w[n * cap : (n + 1) * cap, :] = weight[0:cap, :]
        x = full_ref[0, at, :]
        pre_gate[...] = matmul_nn(x, gate_w[...])
        pre_up[...] = matmul_nn(x, up_w[...])
        back_proj[...] = matmul_nt(full_ref[1, at, :], down_w[...])
        part_cols = 256 if hidden % 256 == 0 else hidden

        def block(b):
            here = pl.ds(pl.multiple_of(b * exact_rows, exact_rows), exact_rows)
            there = pl.ds(
                pl.multiple_of(group * group_rows + b * exact_rows, exact_rows), exact_rows
            )
            weight = slot_w[here, 0:1]
            total = jnp.zeros((exact_rows, 1), F32)
            for c in range(0, hidden, part_cols):
                span = slice(c, c + part_cols)
                gate = pre_gate[here, span]
                up = pre_up[here, span]
                back = back_proj[here, span]
                sigmoid = jax.nn.sigmoid(gate)
                active = gate * sigmoid
                value = active * up
                total = total + jnp.sum(value * back, axis=1, keepdims=True)
                scaled_ref[there, span] = (weight * value).astype(BF16)
                grad = weight * back
                gate_pre[there, span] = (
                    grad * up * sigmoid * (1.0 + gate * (1.0 - sigmoid))
                ).astype(BF16)
                up_pre[there, span] = (grad * active).astype(BF16)
            slot_sum[here, :] = jnp.broadcast_to(total, (exact_rows, 128))

        lax.fori_loop(0, group_rows // exact_rows, lambda b, c: (block(b), c)[1], 0)
        gate_rows = gate_pre[at, :]
        up_rows = up_pre[at, :]
        part_ref[at, :] = (matmul_nt(gate_rows, gate_w[...]) + matmul_nt(up_rows, up_w[...])).astype(
            BF16
        )
        for n in range(size * per):
            column = slot_sum[n * cap : (n + 1) * cap, :]
            block_sum = jnp.concatenate([column, jnp.zeros((128 - cap, 128), F32)], axis=0)
            gate_send_ref[first + n] = jnp.broadcast_to(block_sum.T[0:1, :], (8, 128))

    def send_part(j):
        for i in range(size):
            chunk = chunk_at(j, i)
            for r in range(n_y):
                rcore_copy(lax.rem(y + r + 1, n_y), chunk).start()

    def across(j):
        for i in range(size):
            chunk = chunk_at(j, i)
            here = chunk_rows(chunk)
            for r in range(1, n_y):
                target = lax.rem(y + r, n_y)
                rcore_copy(target, chunk).wait_recv()
                mine = part_ref[here, cols(target * 2 + core)].astype(F32)
                y_out[target, here] = (mine + core_buf[target, here].astype(F32)).astype(BF16)
                ry_copy(y, target, chunk).start()

    def scatter(j):
        for i in range(size):
            chunk = chunk_at(j, i)
            here = chunk_rows(chunk)
            rcore_copy(y, chunk).wait_recv()
            value = part_ref[here, cols(tp)].astype(F32) + core_buf[y, here].astype(F32)
            for r in range(1, n_y):
                source = lax.rem(y + r, n_y)
                ry_copy(source, y, chunk).wait_recv()
                value = value + y_buf[source, here].astype(F32)
            ep_out[here, :] = value.astype(BF16)
            each_source(j, i, lambda dst: rep_copy(dst, ep).start())

    for load in loads:
        load.wait()

    def step(s, carry):
        @pl.when(s < groups)
        def _():
            relay(s)

        @pl.when(s >= 1)
        def _():
            forward(s - 1)
            arrive(s - 1)
            compute(s - 1)
            send_part(s - 1)

        @pl.when(s >= 2)
        def _():
            across(s - 2)

        @pl.when(s >= 3)
        def _():
            scatter(s - 3)

        return carry

    lax.fori_loop(0, groups + 1, step, 0)

    loop(1, n_tp, lambda r: tp_copy(lax.rem(tp + r, n_tp), tp).start())
    gate_buf[tp] = gate_send_ref[...]

    tile = 256 if features % 256 == 0 else features
    tiles = features // tile

    def gate_tile(i, carry):
        span = pl.ds(pl.multiple_of(i * tile, tile), tile)
        x = full_ref[0, :, span]
        for row, (grad, out) in enumerate(((gate_pre, gate_res), (up_pre, up_res))):
            total = matmul_tn(x, grad[...])
            out[0, span, :] = total.astype(BF16)
            square = jnp.sum(total * total, axis=1, keepdims=True)
            square_buf[tp, row : row + 1, span] = jnp.broadcast_to(square, (tile, 128)).T[0:1, :]
        return carry

    down_tile = 256 if hidden % 256 == 0 else hidden
    tangents = full_ref.at[1]

    def down_part(i):
        span = slice(i * down_tile, (i + 1) * down_tile)
        total = matmul_tn(scaled_ref[:, span], tangents[...])
        down_res[0, span, :] = total.astype(BF16)
        square = jnp.sum(total * total, axis=1, keepdims=True)
        down_square_out[0:1, span] = jnp.broadcast_to(square, (down_tile, 128)).T[0:1, :] / features

    split = tiles // 2
    across(groups - 1)
    for i in range(hidden // down_tile):
        down_part(i)
    total = jnp.zeros(gate_send_ref.shape, F32)
    for r in range(1, n_tp):
        tp_copy(tp, lax.rem(tp + r, n_tp)).wait_recv()
    for r in range(n_tp):
        total = total + gate_buf[r]
    gate_back_out[...] = total
    loop(1, n_ep, lambda r: gate_copy(lax.rem(ep + r, n_ep), ep).start())
    gate_back[ep] = gate_back_out[ep]
    for j in range(max(groups - 2, 0), groups):
        scatter(j)
    own_back = pltpu.make_async_copy(
        ep_out.at[source_rows(ep)], back_ref.at[source_rows(ep)], own_sem.at[2]
    )
    own_back.start()
    lax.fori_loop(0, split, gate_tile, 0)

    loop(1, n_ep, lambda r: gate_copy(ep, lax.rem(ep + r, n_ep)).wait_recv())
    routes = routes_ref[...]
    weights = weights_ref[...].astype(F32)
    labels = lax.broadcasted_iota(jnp.int32, (n_ep, tok), 0)
    rest = gate_back[:, 0, :]
    pieces = []
    for _ in range(3):
        pieces.append(rest.astype(BF16).astype(F32))
        rest = rest - pieces[-1]
    picked = matmul_nt(
        jnp.concatenate(pieces, axis=0).astype(BF16), lane_pick(n_ep, cap).astype(BF16)
    )
    mask = own_block(n_ep, cap)
    spread = (picked * jnp.concatenate([mask] * 3, axis=0)).astype(BF16)
    parts = matmul_nn(spread, table_ref[...])
    values = (parts[0:n_ep] + parts[n_ep : 2 * n_ep]) + parts[2 * n_ep :]
    grads = []
    mixed = jnp.zeros((1, tok), F32)
    for k in range(top):
        same = routes[k : k + 1, :] == labels
        grads.append(jnp.sum(jnp.where(same, values, 0.0), axis=0, keepdims=True))
        gate_out[k : k + 1, :] = grads[k]
        mixed = mixed + weights[k : k + 1, :] * grads[k]
    signal = jnp.zeros((n_ep, tok), F32)
    for k in range(top):
        logit = weights[k : k + 1, :] * (grads[k] - mixed)
        signal = signal + jnp.where(routes[k : k + 1, :] == labels, logit, 0.0)
    signal = signal.astype(BF16)
    term = matmul_nn(signal, tokens_ref[...])
    for e in range(n_ep):
        term_ref[e] = term[e : e + 1, :]
    loop(1, n_ep, lambda r: term_copy(lax.rem(ep + r, n_ep), ep).start())
    term_buf[ep] = term_ref[ep]
    lax.fori_loop(split, tiles, gate_tile, 0)
    loop(1, n_tp, lambda r: square_copy(lax.rem(tp + r, n_tp), tp).start())

    own_back.wait()
    loop(1, n_ep, lambda r: rep_copy(ep, lax.rem(ep + r, n_ep)).wait_recv())
    token_out[...] = matmul_tn(table_ref[...], back_ref[...]) + matmul_tn(
        signal, router_ref[:, cols(tp)]
    )
    loop(1, n_ep, lambda r: term_copy(ep, lax.rem(ep + r, n_ep)).wait_recv())
    term_total = term_buf[0]
    for e in range(1, n_ep):
        term_total = term_total + term_buf[e]
    term_out[...] = term_total
    for r in range(1, n_tp):
        square_copy(tp, lax.rem(tp + r, n_tp)).wait_recv()
    square = square_buf[0]
    for r in range(1, n_tp):
        square = square + square_buf[r]
    square_out[...] = square / (hidden * n_tp)

    def drain_ep(r):
        other = lax.rem(ep + r, n_ep)
        for copy in (ep_copy, w_copy, rep_copy, gate_copy, term_copy):
            copy(other, ep).wait_send()

    loop(1, n_ep, drain_ep)

    def drain_tp(r):
        other = lax.rem(tp + r, n_tp)
        tp_copy(other, tp).wait_send()
        square_copy(other, tp).wait_send()

    loop(1, n_tp, drain_tp)

    def drain_chunk(chunk):
        for r in range(n_y):
            core_copy(r, core, chunk).wait_send()
            rcore_copy(r, chunk).wait_send()
        for r in range(1, n_y):
            y_copy(y, lax.rem(y + r, n_y), chunk).wait_send()
            ry_copy(y, lax.rem(y + r, n_y), chunk).wait_send()

    loop(0, chunks, drain_chunk)


def layer(routes, weights, tokens, cotangent, router_rows, gate, up, down, n_ep, n_tp, cap):
    tok, width = tokens.shape
    features, hidden = gate.shape[1:]
    chunks = n_ep if n_ep <= 8 else next(c for c in range(8, 0, -1) if n_ep % c == 0)
    size = 2 if chunks % 2 == 0 else 1
    n_y = n_tp // 2
    slots = n_ep * cap
    group_rows = slots // chunks * size
    dma = pltpu.SemaphoreType.DMA
    in_vmem = pl.BlockSpec(memory_space=VMEM)
    in_hbm = pl.BlockSpec(memory_space=pltpu.HBM)
    return pl.pallas_call(
        functools.partial(layer_kernel, n_ep, n_tp, chunks, cap),
        out_shape=(
            VMEM((tok, width), F32),
            VMEM(routes.shape, F32),
            VMEM((1, width), F32),
            VMEM((2, features), F32),
            VMEM((1, hidden), F32),
            VMEM(gate.shape, BF16),
            VMEM(up.shape, BF16),
            VMEM(down.shape, BF16),
        ),
        in_specs=[in_vmem] * 5 + [in_hbm] * 3,
        out_specs=[in_vmem] * 8,
        scratch_shapes=[
            VMEM((features, hidden), BF16),
            VMEM((features, hidden), BF16),
            VMEM((hidden, features), BF16),
            VMEM((slots, tok), BF16),
            VMEM((2, slots, width), BF16),
            VMEM((n_ep, 8, 128), F32),
            VMEM((2, slots, features), BF16),
            VMEM((n_ep, 8, 128), F32),
            VMEM((group_rows, hidden), F32),
            VMEM((group_rows, hidden), F32),
            VMEM((group_rows, hidden), F32),
            VMEM((group_rows, 128), F32),
            VMEM((group_rows, 128), F32),
            VMEM((slots, hidden), BF16),
            VMEM((slots, hidden), BF16),
            VMEM((slots, hidden), BF16),
            VMEM((slots, features), BF16),
            VMEM((n_ep, 8, 128), F32),
            VMEM((n_tp, n_ep, 8, 128), F32),
            VMEM((n_ep, 8, 128), F32),
            VMEM((n_ep, 8, 128), F32),
            VMEM((n_y, slots, width), BF16),
            VMEM((n_y, slots, width), BF16),
            VMEM((n_y, slots, width), BF16),
            VMEM((slots, width), BF16),
            VMEM((slots, width), BF16),
            VMEM((n_tp, 2, features), F32),
            VMEM((n_ep, 1, width), F32),
            VMEM((n_ep, 1, width), F32),
            dma((3,)),
            dma((3,)),
            dma((n_ep,)),
            dma((n_ep,)),
            dma((n_ep,)),
            dma((n_ep,)),
            dma((n_y, chunks)),
            dma((n_y, chunks)),
            dma((n_y, chunks)),
            dma((n_y, chunks)),
            dma((n_y, chunks)),
            dma((n_y, chunks)),
            dma((n_y, chunks)),
            dma((n_y, chunks)),
            dma((n_ep,)),
            dma((n_ep,)),
            dma((n_tp,)),
            dma((n_tp,)),
            dma((n_ep,)),
            dma((n_ep,)),
            dma((n_tp,)),
            dma((n_tp,)),
            dma((n_ep,)),
            dma((n_ep,)),
        ],
        compiler_params=pltpu.CompilerParams(
            collective_id=0, has_side_effects=True, vmem_limit_bytes=48 * 2**20
        ),
        name="layer",
    )(routes, weights, tokens, cotangent, router_rows, gate, up, down)


def write_kernel(count, *refs):
    ins, outs, sems = refs[:count], refs[count : 2 * count], refs[-1]
    copies = [
        pltpu.make_async_copy(source, target, sems.at[i])
        for i, (source, target) in enumerate(zip(ins, outs, strict=True))
    ]
    for copy in copies:
        copy.start()
    for copy in copies:
        copy.wait()


def write_out(*arrays):
    count = len(arrays)
    return pl.pallas_call(
        functools.partial(write_kernel, count),
        out_shape=tuple(jax.ShapeDtypeStruct(a.shape, a.dtype) for a in arrays),
        in_specs=[pl.BlockSpec(memory_space=VMEM)] * count,
        out_specs=[pl.BlockSpec(memory_space=pltpu.HBM)] * count,
        scratch_shapes=[pltpu.SemaphoreType.DMA((count,))],
        compiler_params=pltpu.CompilerParams(vmem_limit_bytes=2**20),
        name="write_out",
    )(*(pltpu.with_memory_space_constraint(a, VMEM) for a in arrays))


def shards(tokens, routing, gate_weights, cotangent, expert_gate, expert_up, expert_down, router):
    tok_rows = tokens.shape[0]
    top_count = routing.shape[1]
    experts = router.shape[1]
    n_tp = lax.axis_size("tp")
    n_ep = lax.axis_size("ep")
    capacity = 3 * top_count * tok_rows // (2 * experts)
    results = layer(
        routing.T,
        gate_weights.T,
        tokens,
        cotangent,
        router.T,
        expert_gate,
        expert_up,
        expert_down,
        n_ep,
        n_tp,
        capacity,
    )
    token_grad, gate_grad, router_grad, squares, down_squares, gates, ups, downs = write_out(*results)
    return (
        token_grad,
        gate_grad.T,
        gates,
        ups,
        downs,
        router_grad,
        squares[0:1],
        squares[1:2],
        down_squares,
    )


def solution(mesh):
    in_specs = (
        P("ep", "tp"),
        P("ep", None),
        P("ep", None),
        P("ep", "tp"),
        P("ep", None, "tp"),
        P("ep", None, "tp"),
        P("ep", "tp", None),
        P(),
    )
    out_specs = (
        P("ep", "tp"),
        P("ep", None),
        P("ep", None, "tp"),
        P("ep", None, "tp"),
        P("ep", "tp", None),
        P("ep", "tp"),
        P("ep", None),
        P("ep", None),
        P("ep", "tp"),
    )
    return jax.shard_map(shards, mesh=mesh, in_specs=in_specs, out_specs=out_specs, check_vma=False)
```

```python
import functools

import jax
import jax.numpy as jnp
from jax import lax
from jax.experimental import pallas as pl
from jax.experimental.pallas import tpu as pltpu
from jax.sharding import PartitionSpec as P

MESH = pl.DeviceIdType.MESH
F32 = jnp.float32
BF16 = jnp.bfloat16
VMEM = pltpu.VMEM


def matmul_nn(left_side, right_side):
    return jnp.dot(left_side, right_side, preferred_element_type=F32)


def matmul_tn(left_side, right_side):
    return lax.dot_general(
        left_side, right_side, (((0,), (0,)), ((), ())), preferred_element_type=F32
    )


def matmul_nt(left_side, right_side):
    return lax.dot_general(
        left_side, right_side, (((1,), (1,)), ((), ())), preferred_element_type=F32
    )


def loop(lower, upper, body):
    if upper - lower <= 8:
        for i in range(lower, upper):
            body(i)
    else:
        lax.fori_loop(lower, upper, lambda i, carry: (body(i), carry)[1], 0)


def place():
    ep, tp = lax.axis_index("ep"), lax.axis_index("tp")
    return ep, tp, lax.div(tp, 2), lax.rem(tp, 2)


def paired(value, step, count):
    if count & (count - 1):
        return lax.rem(value + step, count)
    out, bit = value, 1
    while bit < count:
        asked = lax.rem(lax.div(jnp.int32(step), bit), 2)
        out = out + asked * bit * (1 - 2 * lax.rem(lax.div(value, bit), 2))
        bit *= 2
    return out


def greet(n_ep, n_tp, between=None):
    ep, tp, _, _ = place()
    barrier = pltpu.get_barrier_semaphore()

    def to_ep(r):
        pl.semaphore_signal(
            barrier, inc=1, device_id=(lax.rem(ep + r, n_ep), tp), device_id_type=MESH
        )

    def to_tp(r):
        pl.semaphore_signal(
            barrier, inc=1, device_id=(ep, lax.rem(tp + r, n_tp)), device_id_type=MESH
        )

    loop(1, n_ep, to_ep)
    loop(1, n_tp, to_tp)
    if between is not None:
        between()
    pl.semaphore_wait(barrier, n_ep - 1 + n_tp - 1)


def lane_pick(n_ep, cap):
    shape = (n_ep, cap, 128)
    pick = lax.broadcasted_iota(jnp.int32, shape, 1) == lax.broadcasted_iota(jnp.int32, shape, 2)
    return pick.astype(F32).reshape(n_ep * cap, 128)


def own_block(n_ep, cap):
    shape = (n_ep, n_ep * cap)
    first = lax.broadcasted_iota(jnp.int32, shape, 0) * cap
    slot = lax.broadcasted_iota(jnp.int32, shape, 1)
    return ((slot >= first) & (slot < first + cap)).astype(F32)


def fill_slots(cap, routes_ref, weights_ref, tokens_ref, cotangent_ref, table_ref, out_ref, w_ref):
    n_ep = w_ref.shape[0]
    width = out_ref.shape[2]
    top, tok = routes_ref.shape
    routes = routes_ref[...]
    weights = weights_ref[...].astype(F32)
    labels = lax.broadcasted_iota(jnp.int32, (n_ep, tok), 0)
    hit = jnp.zeros((n_ep, tok), F32)
    chosen = jnp.zeros((n_ep, tok), F32)
    for k in range(top):
        same = routes[k : k + 1, :] == labels
        hit = hit + same.astype(F32)
        chosen = chosen + jnp.where(same, weights[k : k + 1, :], 0.0)
    square = (tok, tok)
    before = lax.broadcasted_iota(jnp.int32, square, 0) < lax.broadcasted_iota(jnp.int32, square, 1)
    count = matmul_nn(hit.astype(BF16), before.astype(F32).astype(BF16))
    position = jnp.where(hit > 0.0, count, -1.0)
    slot = lax.broadcasted_iota(jnp.int32, (n_ep, cap, tok), 1).astype(F32)
    table = (slot == position[:, None, :]).astype(F32).reshape(n_ep * cap, tok).astype(BF16)
    table_ref[...] = table
    for which, source in enumerate((tokens_ref, cotangent_ref)):
        out_ref[which] = matmul_nn(table, source[...]).astype(BF16)
    spread = matmul_nt(chosen.astype(BF16), table) * own_block(n_ep, cap)
    values = matmul_nn(spread.astype(BF16), lane_pick(n_ep, cap).astype(BF16))
    w_ref[...] = jnp.broadcast_to(values[:, None, :], w_ref.shape)


def layer_kernel(
    n_ep,
    n_tp,
    chunks,
    cap,
    routes_hbm,
    weights_hbm,
    tokens_hbm,
    cotangent_hbm,
    router_hbm,
    gate_hbm,
    up_hbm,
    down_hbm,
    token_out,
    gate_out,
    term_out,
    gate_square_out,
    up_square_out,
    down_square_out,
    gate_res,
    up_res,
    down_res,
    routes_ref,
    weights_ref,
    tokens_ref,
    cotangent_ref,
    router_ref,
    gate_w,
    up_w,
    down_w,
    gate_t,
    up_t,
    down_t,
    table_ref,
    slots_ref,
    w_ref,
    full_ref,
    full_w_ref,
    pre_gate,
    pre_up,
    back_proj,
    slot_w,
    slot_sum,
    scaled_ref,
    gate_pre,
    up_pre,
    part_ref,
    gate_send_ref,
    gate_buf,
    gate_back_out,
    gate_back,
    core_buf,
    y_out,
    y_buf,
    ep_out,
    back_ref,
    square_buf,
    term_ref,
    term_buf,
    load_sem,
    own_sem,
    send_sem,
    all_recv,
    ep_recv,
    y_recv,
    core_recv,
    rcore_recv,
    ry_recv,
):
    ep, tp, y, core = place()
    n_y = n_tp // 2
    partner = y * 2 + 1 - core
    slots, features = part_ref.shape
    width = features // n_tp
    hidden = gate_w.shape[1]
    top, tok = routes_ref.shape
    per = n_ep // chunks
    rows = per * cap
    size = 2 if chunks % 2 == 0 else 1
    groups = chunks // size
    group_rows = size * rows
    exact_rows = 16 if group_rows % 16 == 0 else 8

    batches, backs = batches_of(groups)

    def cols(which):
        return pl.ds(pl.multiple_of(which * width, width), width)

    def y_cols(which):
        return pl.ds(pl.multiple_of(which * (2 * width), 2 * width), 2 * width)

    def base_of(j, count):
        return lax.div(group_at(j), count) * count

    def group_range(j, count, start=0, many=None):
        first = base_of(j, count) * group_rows + start
        return pl.ds(
            pl.multiple_of(first, exact_rows), count * group_rows if many is None else many
        )

    def batch_rows(batch, start=0, many=None):
        return group_range(*batches[batch], start, many)

    def chunk_rows(chunk):
        return pl.ds(pl.multiple_of(chunk * rows, rows), rows)

    def source_rows(source):
        return pl.ds(pl.multiple_of(source * cap, cap), cap)

    def remote(src, dst, send, recv, device):
        return pltpu.make_async_remote_copy(
            src_ref=src,
            dst_ref=dst,
            send_sem=send,
            recv_sem=recv,
            device_id=device,
            device_id_type=MESH,
        )

    def group_at(j):
        return paired(lax.div(ep, per * size), j, groups)

    def chunk_at(j, i):
        return group_at(j) * size + paired(lax.rem(lax.div(ep, per), size), i, size)

    def ep_copy(dst, src):
        return remote(
            slots_ref.at[:, source_rows(dst), :],
            full_ref.at[:, source_rows(src), cols(tp)],
            send_sem.at[0],
            ep_recv.at[src],
            (dst, tp),
        )

    def w_copy(dst, src):
        return remote(w_ref.at[dst], full_w_ref.at[src], send_sem.at[1], all_recv.at[0], (dst, tp))

    def y_copy(source_y, target_y, chunk, r):
        piece = full_ref.at[:, chunk_rows(chunk), cols(source_y * 2 + core)]
        return remote(
            piece, piece, send_sem.at[2], y_recv.at[r - 1, chunk], (ep, target_y * 2 + core)
        )

    def core_copy(source_y, source_core, at, slot, batch):
        piece = full_ref.at[:, at, cols(source_y * 2 + source_core)]
        return remote(piece, piece, send_sem.at[3], core_recv.at[slot, batch], (ep, partner))

    def rcore_copy(target_y, j, count, slot, back):
        at = group_range(j, count)
        return remote(
            part_ref.at[at, cols(target_y * 2 + 1 - core)],
            core_buf.at[target_y, at],
            send_sem.at[4],
            rcore_recv.at[slot, back],
            (ep, partner),
        )

    def ry_copy(source_y, target_y, chunk, r):
        return remote(
            y_out.at[target_y, chunk_rows(chunk)],
            y_buf.at[source_y, chunk_rows(chunk)],
            send_sem.at[5],
            ry_recv.at[r - 1, chunk],
            (ep, target_y * 2 + core),
        )

    def rep_copy(dst, src):
        return remote(
            ep_out.at[source_rows(dst)],
            back_ref.at[source_rows(src)],
            send_sem.at[6],
            all_recv.at[1],
            (dst, tp),
        )

    def tp_copy(dst, src):
        return remote(
            gate_send_ref, gate_buf.at[src], send_sem.at[7], all_recv.at[2], (ep, dst)
        )

    def gate_copy(dst, src):
        return remote(
            gate_back_out.at[dst], gate_back.at[src], send_sem.at[8], all_recv.at[3], (dst, tp)
        )

    def square_copy(dst, src):
        return remote(
            square_buf.at[src], square_buf.at[src], send_sem.at[9], all_recv.at[4], (ep, dst)
        )

    def term_copy(dst, src):
        return remote(
            term_ref.at[dst], term_buf.at[src], send_sem.at[10], all_recv.at[5], (dst, tp)
        )

    def whole(ref, send=None, recv=None):
        copy = remote(
            ref,
            ref,
            send_sem.at[0 if send is None else send],
            all_recv.at[0 if recv is None else recv],
            (ep, partner),
        )
        if send is not None:
            copy.wait_send()
        if recv is not None:
            copy.wait_recv()

    others = n_ep - 1

    pairs = (
        (routes_hbm, routes_ref),
        (weights_hbm, weights_ref),
        (tokens_hbm, tokens_ref),
        (cotangent_hbm, cotangent_ref),
        (gate_hbm.at[0], gate_w),
        (up_hbm.at[0], up_w),
        (down_hbm.at[0], down_w),
        (router_hbm, router_ref),
    )
    loads = [pltpu.make_async_copy(*pair, load_sem.at[i]) for i, pair in enumerate(pairs)]

    def begin():
        for load in loads:
            load.start()
        for load in loads[:4]:
            load.wait()
        fill()

    fill = functools.partial(
        fill_slots,
        cap,
        routes_ref,
        weights_ref,
        tokens_ref,
        cotangent_ref,
        table_ref,
        slots_ref,
        w_ref,
    )
    greet(n_ep, n_tp, begin)

    own_rows = pltpu.make_async_copy(
        slots_ref.at[:, source_rows(ep), :],
        full_ref.at[:, source_rows(ep), cols(tp)],
        own_sem.at[0],
    )
    own_w = pltpu.make_async_copy(w_ref.at[ep], full_w_ref.at[ep], own_sem.at[1])
    own_rows.start()
    own_w.start()

    def each_source(j, i, body):
        chunk = chunk_at(j, i)

        def one(n):
            source = chunk * per + n

            @pl.when(source != ep)
            def _():
                body(source)

        loop(0, per, one)

    def send_group(j):
        for i in range(size):
            each_source(j, i, lambda dst: ep_copy(dst, ep).start())

    loop(1, n_ep, lambda r: w_copy(lax.rem(ep + r, n_ep), ep).start())
    loop(0, groups, send_group)
    gate_send_ref[...] = jnp.zeros_like(gate_send_ref)
    own_rows.wait()
    own_w.wait()

    def batch_of(j):
        return next(b for b, (k, count) in enumerate(batches) if k <= j < k + count)

    def relay(j, i):
        chunk = chunk_at(j, i)
        each_source(j, i, lambda source: ep_copy(ep, source).wait_recv())
        for r in range(1, n_y):
            y_copy(y, lax.rem(y + r, n_y), chunk, r).start()
        core_copy(y, core, chunk_rows(chunk), 0, batch_of(j)).start()

    def forward(j, i):
        chunk = chunk_at(j, i)
        for r in range(1, n_y):
            source_y = lax.rem(y + n_y - r, n_y)
            y_copy(source_y, y, chunk, r).wait_recv()
            core_copy(source_y, core, chunk_rows(chunk), r, batch_of(j)).start()

    def chunks_of(batch):
        j, count = batches[batch]
        return [(k, i) for k in range(j, j + count) for i in range(size)]

    def back_chunks(back):
        j, count = backs[back]
        return [(k, i) for k in range(j, j + count) for i in range(size)]

    def multiply(batch, which, first):
        at = batch_rows(batch)
        many = batches[batch][1] * group_rows
        k = y_cols(which)
        x, t = full_ref[0, at, k], full_ref[1, at, k]
        for out, value in (
            (pre_gate, matmul_nn(x, gate_w[k, :])),
            (pre_up, matmul_nn(x, up_w[k, :])),
            (back_proj, matmul_nn(t, down_t[k, :])),
        ):
            out[0:many, :] = value if first else out[0:many, :] + value

    def near_product(batch):
        core_copy(y, 1 - core, batch_rows(batch), 0, batch).wait_recv()
        multiply(batch, y, True)

    def far_product(batch):
        for r in range(1, n_y):
            source_y = lax.rem(y + n_y - r, n_y)
            core_copy(source_y, 1 - core, batch_rows(batch), r, batch).wait_recv()
            multiply(batch, source_y, False)

    part_cols = 256 if hidden % 256 == 0 else hidden
    lane_sums = part_cols % 128 == 0
    first_lane = lax.broadcasted_iota(jnp.int32, (exact_rows, 128), 1) == 0

    def gradients(batch):
        first = base_of(*batches[batch]) * (size * per)
        many = batches[batch][1] * size * per
        for n in range(many):
            weight = jnp.broadcast_to(full_w_ref[first + n][0:1, :], (128, 128)).T
            slot_w[n * cap : (n + 1) * cap, :] = weight[0:cap, :]
        for b in range(0, many * cap, exact_rows):
            here = slice(b, b + exact_rows)
            there = batch_rows(batch, b, exact_rows)
            weight = slot_w[here, 0:1]
            total = jnp.zeros((exact_rows, 128), F32)
            for c in range(0, hidden, part_cols):
                span = slice(c, c + part_cols)
                gate = pre_gate[here, span]
                up = pre_up[here, span]
                back = back_proj[here, span]
                sigmoid = 0.5 * jnp.tanh(0.5 * gate) + 0.5
                active = gate * sigmoid
                value = active * up
                product = value * back
                if lane_sums:
                    for lane in range(0, part_cols, 128):
                        total = total + product[:, lane : lane + 128]
                else:
                    row = jnp.sum(product, axis=1, keepdims=True)
                    total = total + jnp.where(first_lane, row, 0.0)
                scaled_ref[there, span] = (weight * value).astype(BF16)
                grad = weight * back
                gate_pre[there, span] = (
                    grad * up * (sigmoid * (1.0 + gate * (1.0 - sigmoid)))
                ).astype(BF16)
                up_pre[there, span] = (grad * active).astype(BF16)
            slot_sum[here, :] = jnp.broadcast_to(
                jnp.sum(total, axis=1, keepdims=True), (exact_rows, 128)
            )
        for n in range(many):
            column = slot_sum[n * cap : (n + 1) * cap, :]
            block_sum = jnp.concatenate([column, jnp.zeros((128 - cap, 128), F32)], axis=0)
            gate_send_ref[first + n] = jnp.broadcast_to(block_sum.T[0:1, :], (8, 128))

    def slot_grads(back, r, own):
        j, count = backs[back]
        at = group_range(j, count)
        target = lax.rem(y + r, n_y)
        block = cols(target * 2 + (core if own else 1 - core))
        part_ref[at, block] = (
            matmul_nn(gate_pre[at, :], gate_t[:, block]) + matmul_nn(up_pre[at, :], up_t[:, block])
        ).astype(BF16)
        if not own:
            rcore_copy(target, j, count, r, back).start()

    def across(back):
        for r in range(1, n_y):
            target = lax.rem(y + r, n_y)
            rcore_copy(target, *backs[back], r, back).wait_recv()
            for j, i in back_chunks(back):
                chunk = chunk_at(j, i)
                here = chunk_rows(chunk)
                mine = part_ref[here, cols(target * 2 + core)].astype(F32)
                y_out[target, here] = (mine + core_buf[target, here].astype(F32)).astype(BF16)
                ry_copy(y, target, chunk, r).start()

    def own_arrives(back):
        rcore_copy(y, *backs[back], 0, back).wait_recv()

    def scatter(j, i):
        chunk = chunk_at(j, i)
        here = chunk_rows(chunk)
        value = part_ref[here, cols(tp)].astype(F32) + core_buf[y, here].astype(F32)
        for r in range(1, n_y):
            source = lax.rem(y + n_y - r, n_y)
            ry_copy(source, y, chunk, r).wait_recv()
            value = value + y_buf[source, here].astype(F32)
        ep_out[here, :] = value.astype(BF16)
        each_source(j, i, lambda dst: rep_copy(dst, ep).start())

    for load in loads[4:]:
        load.wait()

    def each(chosen, body):
        for j, i in chosen:
            body(j, i)

    def slots_other(back):
        for r in range(1, n_y):
            slot_grads(back, r, False)
            slot_grads(back, r, True)

    def slots_own(back):
        slot_grads(back, 0, False)
        across(back)
        slot_grads(back, 0, True)

    def prep_tile(source, target, turns):
        def turn(i, carry):
            span = pl.ds(pl.multiple_of(i * 256, 256), 256)
            target[:, span] = source[span, :].T
            return carry

        lax.fori_loop(0, turns, turn, 0)

    def prep_down():
        span = 256 if hidden % 256 == 0 else hidden
        for c in range(0, hidden, span):
            down_t[:, c : c + span] = down_w[c : c + span, :].T

    prep_down()
    last = len(batches) - 1
    ready = {k + count - 1: b for b, (k, count) in enumerate(backs)}
    each(chunks_of(0)[:2], relay)
    prep_tile(gate_w, gate_t, features // 256)
    each(chunks_of(0)[2:], relay)
    prep_tile(up_w, up_t, features // 256)
    near_product(0)
    whole(full_w_ref.at[pl.ds(0, others)], recv=0)
    pending = None
    for b in range(last):
        later = chunks_of(b + 1)
        if b == 0:
            each(later[:1], relay)
            each(chunks_of(0), forward)
            each(later[1:], relay)
        far_product(b)
        gradients(b)
        near_product(b + 1)
        after = chunks_of(b + 2) if b + 2 <= last else []
        each(after[:1], relay)
        each(later, forward)
        if pending is not None:
            slots_own(pending)
            pending = None
        done = ready.get(sum(batches[b]) - 1)
        if done is not None:
            slots_other(done)
            pending = done
        each(after[1:], relay)
    if pending is not None:
        slots_own(pending)
    if last == 0:
        each(chunks_of(0), forward)
    far_product(last)
    gradients(last)
    loop(1, n_tp, lambda r: tp_copy(lax.rem(tp + r, n_tp), tp).start())
    gate_buf[tp] = gate_send_ref[...]
    final = len(backs) - 1
    slots_other(final)

    def add_gates():
        whole(gate_buf.at[pl.ds(0, n_tp - 1)], recv=2)
        total = gate_buf[0]
        for r in range(1, n_tp):
            total = total + gate_buf[r]
        gate_back_out[...] = total
        loop(1, n_ep, lambda r: gate_copy(lax.rem(ep + r, n_ep), ep).start())
        gate_back[ep] = gate_back_out[ep]

    slots_own(final)

    tile = 256 if features % 256 == 0 else features
    tiles = features // tile

    def gate_tile(i, carry):
        span = pl.ds(pl.multiple_of(i * tile, tile), tile)
        x = full_ref[0, :, span]
        for row, (grad, out) in enumerate(((gate_pre, gate_res), (up_pre, up_res))):
            total = matmul_tn(x, grad[...])
            out[0, span, :] = total.astype(BF16)
            square = jnp.sum(total * total, axis=1, keepdims=True)
            square_buf[tp, row : row + 1, span] = jnp.broadcast_to(square, (tile, 128)).T[0:1, :]
        return carry

    down_tile = 256 if hidden % 256 == 0 else hidden
    tangents = full_ref.at[1]

    def down_part(i):
        span = slice(i * down_tile, (i + 1) * down_tile)
        total = matmul_tn(scaled_ref[:, span], tangents[...])
        down_res[0, span, :] = total.astype(BF16)
        square = jnp.sum(total * total, axis=1, keepdims=True)
        down_square_out[0:1, span] = jnp.broadcast_to(square, (down_tile, 128)).T[0:1, :] / features

    early = min(2, tiles)
    middle = min(tiles, early + 2)
    chosen = back_chunks(final)
    half = (len(chosen) + 1) // 2
    for b in range(final):
        own_arrives(b)
        each(back_chunks(b), scatter)
    lax.fori_loop(0, 1, gate_tile, 0)
    add_gates()
    lax.fori_loop(1, early, gate_tile, 0)
    own_arrives(final)
    each(chosen[:half], scatter)
    lax.fori_loop(early, middle, gate_tile, 0)

    whole(gate_back.at[pl.ds(0, others)], recv=3)
    routes = routes_ref[...]
    weights = weights_ref[...].astype(F32)
    labels = lax.broadcasted_iota(jnp.int32, (n_ep, tok), 0)
    rest = gate_back[:, 0, :]
    pieces = []
    for _ in range(3):
        pieces.append(rest.astype(BF16).astype(F32))
        rest = rest - pieces[-1]
    picked = matmul_nt(
        jnp.concatenate(pieces, axis=0).astype(BF16), lane_pick(n_ep, cap).astype(BF16)
    )
    mask = own_block(n_ep, cap)
    spread = (picked * jnp.concatenate([mask] * 3, axis=0)).astype(BF16)
    parts = matmul_nn(spread, table_ref[...])
    values = (parts[0:n_ep] + parts[n_ep : 2 * n_ep]) + parts[2 * n_ep :]
    grads = []
    mixed = jnp.zeros((1, tok), F32)
    for k in range(top):
        same = routes[k : k + 1, :] == labels
        grads.append(jnp.sum(jnp.where(same, values, 0.0), axis=0, keepdims=True))
        gate_out[k : k + 1, :] = grads[k]
        mixed = mixed + weights[k : k + 1, :] * grads[k]
    signal = jnp.zeros((n_ep, tok), F32)
    for k in range(top):
        logit = weights[k : k + 1, :] * (grads[k] - mixed)
        signal = signal + jnp.where(routes[k : k + 1, :] == labels, logit, 0.0)
    signal = signal.astype(BF16)
    term = matmul_nn(signal, tokens_ref[...])
    for e in range(n_ep):
        term_ref[e] = term[e : e + 1, :]
    loop(1, n_ep, lambda r: term_copy(lax.rem(ep + r, n_ep), ep).start())
    term_buf[ep] = term_ref[ep]
    each(chosen[half:], scatter)
    own_back = pltpu.make_async_copy(
        ep_out.at[source_rows(ep)], back_ref.at[source_rows(ep)], own_sem.at[2]
    )
    own_back.start()
    lax.fori_loop(middle, tiles, gate_tile, 0)
    loop(1, n_tp, lambda r: square_copy(lax.rem(tp + r, n_tp), tp).start())
    for i in range(hidden // down_tile):
        down_part(i)
    part_slots = pl.ds(0, others * cap)
    whole(slots_ref.at[:, part_slots], send=0)
    whole(full_w_ref.at[pl.ds(0, others)], send=1)
    whole(full_ref.at[:, :, pl.ds(0, (n_y - 1) * width)], send=2)
    whole(full_ref.at[:, :, pl.ds(0, n_y * width)], send=3)
    whole(core_buf, send=4)
    whole(y_out.at[pl.ds(0, n_y - 1)], send=5)
    whole(gate_buf.at[pl.ds(0, n_tp - 1)], send=7)
    whole(gate_back.at[pl.ds(0, others)], send=8)
    whole(square_buf.at[pl.ds(0, n_tp - 1)], send=9)

    own_back.wait()
    whole(back_ref.at[part_slots], recv=1)
    token_out[...] = matmul_tn(table_ref[...], back_ref[...]) + matmul_tn(
        signal, router_ref[:, cols(tp)]
    )
    whole(term_buf.at[pl.ds(0, others)], recv=5)
    term_total = term_buf[0]
    for e in range(1, n_ep):
        term_total = term_total + term_buf[e]
    term_out[...] = term_total
    whole(square_buf.at[pl.ds(0, n_tp - 1)], recv=4)
    square = square_buf[0]
    for r in range(1, n_tp):
        square = square + square_buf[r]
    square = square / (hidden * n_tp)
    gate_square_out[...] = square[0:1, :]
    up_square_out[...] = square[1:2, :]

    whole(back_ref.at[part_slots], send=6)
    whole(term_buf.at[pl.ds(0, others)], send=10)


def batches_of(groups):
    if groups == 4:
        return ((0, 2), (2, 1), (3, 1)), ((0, 2), (2, 2))
    single = tuple((j, 1) for j in range(groups))
    return single, single


def layer(routes, weights, tokens, cotangent, router_rows, gate, up, down, n_ep, n_tp, cap):
    tok, width = tokens.shape
    features, hidden = gate.shape[1:]
    chunks = n_ep if n_ep <= 8 else next(c for c in range(8, 0, -1) if n_ep % c == 0)
    size = 2 if chunks % 2 == 0 else 1
    n_y = n_tp // 2
    slots = n_ep * cap
    batches, backs = batches_of(chunks // size)
    batch_rows = slots // chunks * size * max(count for _, count in batches)
    dma = pltpu.SemaphoreType.DMA
    in_vmem = pl.BlockSpec(memory_space=VMEM)
    in_hbm = pl.BlockSpec(memory_space=pltpu.HBM)
    return pl.pallas_call(
        functools.partial(layer_kernel, n_ep, n_tp, chunks, cap),
        out_shape=(
            VMEM((tok, width), F32),
            VMEM(routes.shape, F32),
            VMEM((1, width), F32),
            VMEM((1, features), F32),
            VMEM((1, features), F32),
            VMEM((1, hidden), F32),
            VMEM(gate.shape, BF16),
            VMEM(up.shape, BF16),
            VMEM(down.shape, BF16),
        ),
        in_specs=[in_hbm] * 8,
        out_specs=[in_vmem] * 9,
        scratch_shapes=[
            VMEM(routes.shape, routes.dtype),
            VMEM(weights.shape, BF16),
            VMEM(tokens.shape, BF16),
            VMEM(tokens.shape, BF16),
            VMEM(router_rows.shape, BF16),
            VMEM((features, hidden), BF16),
            VMEM((features, hidden), BF16),
            VMEM((hidden, features), BF16),
            VMEM((hidden, features), BF16),
            VMEM((hidden, features), BF16),
            VMEM((features, hidden), BF16),
            VMEM((slots, tok), BF16),
            VMEM((2, slots, width), BF16),
            VMEM((n_ep, 8, 128), F32),
            VMEM((2, slots, features), BF16),
            VMEM((n_ep, 8, 128), F32),
            VMEM((batch_rows, hidden), F32),
            VMEM((batch_rows, hidden), F32),
            VMEM((batch_rows, hidden), F32),
            VMEM((batch_rows, 128), F32),
            VMEM((batch_rows, 128), F32),
            VMEM((slots, hidden), BF16),
            VMEM((slots, hidden), BF16),
            VMEM((slots, hidden), BF16),
            VMEM((slots, features), BF16),
            VMEM((n_ep, 8, 128), F32),
            VMEM((n_tp, n_ep, 8, 128), F32),
            VMEM((n_ep, 8, 128), F32),
            VMEM((n_ep, 8, 128), F32),
            VMEM((n_y, slots, width), BF16),
            VMEM((n_y, slots, width), BF16),
            VMEM((n_y, slots, width), BF16),
            VMEM((slots, width), BF16),
            VMEM((slots, width), BF16),
            VMEM((n_tp, 2, features), F32),
            VMEM((n_ep, 1, width), F32),
            VMEM((n_ep, 1, width), F32),
            dma((8,)),
            dma((3,)),
            dma((11,)),
            dma((6,)),
            dma((n_ep,)),
            dma((n_y - 1, chunks)),
            dma((n_y, len(batches))),
            dma((n_y, len(backs))),
            dma((n_y - 1, chunks)),
        ],
        compiler_params=pltpu.CompilerParams(
            collective_id=0, has_side_effects=True, vmem_limit_bytes=48 * 2**20
        ),
        name="layer",
    )(routes, weights, tokens, cotangent, router_rows, gate, up, down)


def write_kernel(count, *refs):
    ins, outs, sems = refs[:count], refs[count : 2 * count], refs[-1]
    copies = [
        pltpu.make_async_copy(source, target, sems.at[i])
        for i, (source, target) in enumerate(zip(ins, outs, strict=True))
    ]
    for copy in copies:
        copy.start()
    for copy in copies:
        copy.wait()


def write_out(*arrays):
    count = len(arrays)
    return pl.pallas_call(
        functools.partial(write_kernel, count),
        out_shape=tuple(jax.ShapeDtypeStruct(a.shape, a.dtype) for a in arrays),
        in_specs=[pl.BlockSpec(memory_space=VMEM)] * count,
        out_specs=[pl.BlockSpec(memory_space=pltpu.HBM)] * count,
        scratch_shapes=[pltpu.SemaphoreType.DMA((count,))],
        compiler_params=pltpu.CompilerParams(vmem_limit_bytes=2**20),
        name="write_out",
    )(*(pltpu.with_memory_space_constraint(a, VMEM) for a in arrays))


def shards(tokens, routing, gate_weights, cotangent, expert_gate, expert_up, expert_down, router):
    tok_rows = tokens.shape[0]
    top_count = routing.shape[1]
    experts = router.shape[1]
    n_tp = lax.axis_size("tp")
    n_ep = lax.axis_size("ep")
    capacity = 3 * top_count * tok_rows // (2 * experts)
    results = layer(
        routing.T,
        gate_weights.T,
        tokens,
        cotangent,
        router.T,
        expert_gate,
        expert_up,
        expert_down,
        n_ep,
        n_tp,
        capacity,
    )
    token_grad, gate_grad, router_grad, gate_square, up_square, down_square, gates, ups, downs = (
        write_out(*results)
    )
    return (
        token_grad,
        gate_grad.T,
        gates,
        ups,
        downs,
        router_grad,
        gate_square,
        up_square,
        down_square,
    )


def solution(mesh):
    in_specs = (
        P("ep", "tp"),
        P("ep", None),
        P("ep", None),
        P("ep", "tp"),
        P("ep", None, "tp"),
        P("ep", None, "tp"),
        P("ep", "tp", None),
        P(),
    )
    out_specs = (
        P("ep", "tp"),
        P("ep", None),
        P("ep", None, "tp"),
        P("ep", None, "tp"),
        P("ep", "tp", None),
        P("ep", "tp"),
        P("ep", None),
        P("ep", None),
        P("ep", "tp"),
    )
    return jax.shard_map(shards, mesh=mesh, in_specs=in_specs, out_specs=out_specs, check_vma=False)
```

```python
import functools

import jax
import jax.numpy as jnp
from jax import lax
from jax.experimental import pallas as pl
from jax.experimental.pallas import tpu as pltpu
from jax.sharding import PartitionSpec as P

MESH = pl.DeviceIdType.MESH
F32 = jnp.float32
BF16 = jnp.bfloat16
VMEM = pltpu.VMEM


def matmul_nn(left_side, right_side):
    return jnp.dot(left_side, right_side, preferred_element_type=F32)


def matmul_tn(left_side, right_side):
    return lax.dot_general(
        left_side, right_side, (((0,), (0,)), ((), ())), preferred_element_type=F32
    )


def matmul_nt(left_side, right_side):
    return lax.dot_general(
        left_side, right_side, (((1,), (1,)), ((), ())), preferred_element_type=F32
    )


def loop(lower, upper, body):
    if upper - lower <= 8:
        for i in range(lower, upper):
            body(i)
    else:
        lax.fori_loop(lower, upper, lambda i, carry: (body(i), carry)[1], 0)


def place():
    ep, tp = lax.axis_index("ep"), lax.axis_index("tp")
    return ep, tp, lax.div(tp, 2), lax.rem(tp, 2)


def paired(value, step, count):
    if count & (count - 1):
        return lax.rem(value + step, count)
    out, bit = value, 1
    while bit < count:
        asked = lax.rem(lax.div(jnp.int32(step), bit), 2)
        out = out + asked * bit * (1 - 2 * lax.rem(lax.div(value, bit), 2))
        bit *= 2
    return out


def greet(n_ep, n_tp, between=None):
    ep, tp, _, _ = place()
    barrier = pltpu.get_barrier_semaphore()

    def to_ep(r):
        pl.semaphore_signal(
            barrier, inc=1, device_id=(lax.rem(ep + r, n_ep), tp), device_id_type=MESH
        )

    def to_tp(r):
        pl.semaphore_signal(
            barrier, inc=1, device_id=(ep, lax.rem(tp + r, n_tp)), device_id_type=MESH
        )

    loop(1, n_ep, to_ep)
    loop(1, n_tp, to_tp)
    if between is not None:
        between()
    pl.semaphore_wait(barrier, n_ep - 1 + n_tp - 1)


def lane_pick(n_ep, cap):
    shape = (n_ep, cap, 128)
    pick = lax.broadcasted_iota(jnp.int32, shape, 1) == lax.broadcasted_iota(jnp.int32, shape, 2)
    return pick.astype(F32).reshape(n_ep * cap, 128)


def own_block(n_ep, cap):
    shape = (n_ep, n_ep * cap)
    first = lax.broadcasted_iota(jnp.int32, shape, 0) * cap
    slot = lax.broadcasted_iota(jnp.int32, shape, 1)
    return ((slot >= first) & (slot < first + cap)).astype(F32)


def fill_slots(cap, routes_ref, weights_ref, tokens_ref, cotangent_ref, table_ref, out_ref, w_ref):
    n_ep = w_ref.shape[0]
    width = out_ref.shape[2]
    top, tok = routes_ref.shape
    routes = routes_ref[...]
    weights = weights_ref[...].astype(F32)
    labels = lax.broadcasted_iota(jnp.int32, (n_ep, tok), 0)
    hit = jnp.zeros((n_ep, tok), F32)
    chosen = jnp.zeros((n_ep, tok), F32)
    for k in range(top):
        same = routes[k : k + 1, :] == labels
        hit = hit + same.astype(F32)
        chosen = chosen + jnp.where(same, weights[k : k + 1, :], 0.0)
    square = (tok, tok)
    before = lax.broadcasted_iota(jnp.int32, square, 0) < lax.broadcasted_iota(jnp.int32, square, 1)
    count = matmul_nn(hit.astype(BF16), before.astype(F32).astype(BF16))
    position = jnp.where(hit > 0.0, count, -1.0)
    slot = lax.broadcasted_iota(jnp.int32, (n_ep, cap, tok), 1).astype(F32)
    table = (slot == position[:, None, :]).astype(F32).reshape(n_ep * cap, tok).astype(BF16)
    table_ref[...] = table
    for which, source in enumerate((tokens_ref, cotangent_ref)):
        out_ref[which] = matmul_nn(table, source[...]).astype(BF16)
    spread = matmul_nt(chosen.astype(BF16), table) * own_block(n_ep, cap)
    values = matmul_nn(spread.astype(BF16), lane_pick(n_ep, cap).astype(BF16))
    for e in range(n_ep):
        w_ref[e] = values[e : e + 1, :]


def layer_kernel(
    n_ep,
    n_tp,
    chunks,
    cap,
    routes_hbm,
    weights_hbm,
    tokens_hbm,
    cotangent_hbm,
    gate_hbm,
    up_hbm,
    down_hbm,
    gate_res,
    up_res,
    down_res,
    back_ref,
    table_ref,
    signal_out,
    term_buf,
    square_buf,
    gate_out,
    down_square_out,
    routes_ref,
    weights_ref,
    tokens_ref,
    cotangent_ref,
    gate_w,
    up_w,
    down_w,
    gate_t,
    up_t,
    down_t,
    slots_ref,
    w_ref,
    full_ref,
    full_w_ref,
    pre_gate,
    pre_up,
    back_proj,
    slot_w,
    slot_sum,
    scaled_ref,
    gate_pre,
    up_pre,
    part_ref,
    gate_send_ref,
    gate_buf,
    gate_back_out,
    gate_back,
    core_buf,
    y_out,
    y_buf,
    ep_out,
    term_ref,
    load_sem,
    own_sem,
    send_sem,
    all_recv,
    ep_recv,
    y_recv,
    core_recv,
    rcore_recv,
    ry_recv,
):
    ep, tp, y, core = place()
    n_y = n_tp // 2
    partner = y * 2 + 1 - core
    slots, features = part_ref.shape
    width = features // n_tp
    hidden = gate_w.shape[1]
    top, tok = routes_ref.shape
    per = n_ep // chunks
    rows = per * cap
    size = 2 if chunks % 2 == 0 else 1
    groups = chunks // size
    group_rows = size * rows
    exact_rows = 16 if group_rows % 16 == 0 else 8

    batches = batches_of(groups)

    def cols(which):
        return pl.ds(pl.multiple_of(which * width, width), width)

    def y_cols(which):
        return pl.ds(pl.multiple_of(which * (2 * width), 2 * width), 2 * width)

    def base_of(j, count):
        return lax.div(group_at(j), count) * count

    def group_range(j, count, start=0, many=None):
        first = base_of(j, count) * group_rows + start
        return pl.ds(
            pl.multiple_of(first, exact_rows), count * group_rows if many is None else many
        )

    def batch_rows(batch, start=0, many=None):
        return group_range(*batches[batch], start, many)

    def chunk_rows(chunk):
        return pl.ds(pl.multiple_of(chunk * rows, rows), rows)

    def source_rows(source):
        return pl.ds(pl.multiple_of(source * cap, cap), cap)

    def remote(src, dst, send, recv, device):
        return pltpu.make_async_remote_copy(
            src_ref=src,
            dst_ref=dst,
            send_sem=send,
            recv_sem=recv,
            device_id=device,
            device_id_type=MESH,
        )

    def group_at(j):
        return paired(lax.div(ep, per * size), j, groups)

    def chunk_at(j, i):
        return group_at(j) * size + paired(lax.rem(lax.div(ep, per), size), i, size)

    def ep_copy(dst, src, part):
        return remote(
            slots_ref.at[part, source_rows(dst), :],
            full_ref.at[part, source_rows(src), cols(tp)],
            send_sem.at[0],
            ep_recv.at[part, src],
            (dst, tp),
        )

    def w_copy(dst, src):
        return remote(w_ref.at[dst], full_w_ref.at[src], send_sem.at[1], all_recv.at[0], (dst, tp))

    def y_copy(source_y, target_y, chunk, r, part):
        piece = full_ref.at[part, chunk_rows(chunk), cols(source_y * 2 + core)]
        return remote(
            piece, piece, send_sem.at[2], y_recv.at[r - 1, part, chunk], (ep, target_y * 2 + core)
        )

    def core_copy(source_y, source_core, at, slot, batch, part):
        piece = full_ref.at[part, at, cols(source_y * 2 + source_core)]
        return remote(piece, piece, send_sem.at[3], core_recv.at[slot, part, batch], (ep, partner))

    def rcore_copy(target_y, j, count, slot, back):
        at = group_range(j, count)
        return remote(
            part_ref.at[at, cols(target_y * 2 + 1 - core)],
            core_buf.at[target_y, at],
            send_sem.at[4],
            rcore_recv.at[slot, back],
            (ep, partner),
        )

    def ry_copy(source_y, target_y, chunk, r):
        return remote(
            y_out.at[target_y, chunk_rows(chunk)],
            y_buf.at[source_y, chunk_rows(chunk)],
            send_sem.at[5],
            ry_recv.at[r - 1, chunk],
            (ep, target_y * 2 + core),
        )

    def rep_copy(dst, src):
        return remote(
            ep_out.at[source_rows(dst)],
            back_ref.at[source_rows(src)],
            send_sem.at[6],
            all_recv.at[1],
            (dst, tp),
        )

    def tp_copy(dst, src):
        return remote(
            gate_send_ref, gate_buf.at[src], send_sem.at[7], all_recv.at[2], (ep, dst)
        )

    def gate_copy(dst, src):
        return remote(
            gate_back_out.at[dst], gate_back.at[src], send_sem.at[8], all_recv.at[3], (dst, tp)
        )

    def square_copy(dst, src):
        return remote(
            square_buf.at[src], square_buf.at[src], send_sem.at[9], all_recv.at[4], (ep, dst)
        )

    def term_copy(dst, src):
        return remote(
            term_ref.at[dst], term_buf.at[src], send_sem.at[10], all_recv.at[5], (dst, tp)
        )

    def whole(ref, send=None, recv=None):
        copy = remote(
            ref,
            ref,
            send_sem.at[0 if send is None else send],
            all_recv.at[0 if recv is None else recv],
            (ep, partner),
        )
        if send is not None:
            copy.wait_send()
        if recv is not None:
            copy.wait_recv()

    others = n_ep - 1

    pairs = (
        (routes_hbm, routes_ref),
        (weights_hbm, weights_ref),
        (tokens_hbm, tokens_ref),
        (cotangent_hbm, cotangent_ref),
        (gate_hbm.at[0], gate_w),
        (up_hbm.at[0], up_w),
        (down_hbm.at[0], down_w),
    )
    loads = [pltpu.make_async_copy(*pair, load_sem.at[i]) for i, pair in enumerate(pairs)]

    def begin():
        for load in loads:
            load.start()
        for load in loads[:4]:
            load.wait()
        fill()

    fill = functools.partial(
        fill_slots,
        cap,
        routes_ref,
        weights_ref,
        tokens_ref,
        cotangent_ref,
        table_ref,
        slots_ref,
        w_ref,
    )
    greet(n_ep, n_tp, begin)

    own_rows = pltpu.make_async_copy(
        slots_ref.at[:, source_rows(ep), :],
        full_ref.at[:, source_rows(ep), cols(tp)],
        own_sem.at[0],
    )
    own_w = pltpu.make_async_copy(w_ref.at[ep], full_w_ref.at[ep], own_sem.at[1])
    own_rows.start()
    own_w.start()

    def each_source(j, i, body):
        chunk = chunk_at(j, i)

        def one(n):
            source = chunk * per + n

            @pl.when(source != ep)
            def _():
                body(source)

        loop(0, per, one)

    def send_group(j):
        for i in range(size):
            for part in range(2):
                each_source(j, i, lambda dst: ep_copy(dst, ep, part).start())

    loop(1, n_ep, lambda r: w_copy(lax.rem(ep + r, n_ep), ep).start())
    loop(0, groups, send_group)
    gate_send_ref[...] = jnp.zeros_like(gate_send_ref)
    own_rows.wait()
    own_w.wait()

    def batch_of(j):
        return next(b for b, (k, count) in enumerate(batches) if k <= j < k + count)

    def relay(j, i):
        chunk = chunk_at(j, i)
        for part in range(2):
            each_source(j, i, lambda source: ep_copy(ep, source, part).wait_recv())
            for r in range(1, n_y):
                y_copy(y, lax.rem(y + r, n_y), chunk, r, part).start()
            core_copy(y, core, chunk_rows(chunk), 0, batch_of(j), part).start()

    def forward(j, i):
        chunk = chunk_at(j, i)
        for part in range(2):
            for r in range(1, n_y):
                source_y = lax.rem(y + n_y - r, n_y)
                y_copy(source_y, y, chunk, r, part).wait_recv()
                core_copy(source_y, core, chunk_rows(chunk), r, batch_of(j), part).start()

    def chunks_of(batch):
        j, count = batches[batch]
        return [(k, i) for k in range(j, j + count) for i in range(size)]

    def product(batch, source_y, slot):
        at = batch_rows(batch)
        many = batches[batch][1] * group_rows
        k = y_cols(source_y)

        def put(out, value):
            out[0:many, :] = value if slot == 0 else out[0:many, :] + value

        core_copy(source_y, 1 - core, at, slot, batch, 0).wait_recv()
        put(pre_gate, matmul_nn(full_ref[0, at, k], gate_w[k, :]))
        put(pre_up, matmul_nn(full_ref[0, at, k], up_w[k, :]))
        core_copy(source_y, 1 - core, at, slot, batch, 1).wait_recv()
        put(back_proj, matmul_nn(full_ref[1, at, k], down_t[k, :]))

    def near_product(batch):
        product(batch, y, 0)

    def far_product(batch):
        for r in range(1, n_y):
            product(batch, lax.rem(y + n_y - r, n_y), r)

    part_cols = 256 if hidden % 256 == 0 else hidden
    lane_sums = part_cols % 128 == 0
    first_lane = lax.broadcasted_iota(jnp.int32, (exact_rows, 128), 1) == 0

    def gradients(batch):
        first = base_of(*batches[batch]) * (size * per)
        many = batches[batch][1] * size * per
        for n in range(many):
            weight = jnp.broadcast_to(full_w_ref[first + n], (128, 128)).T
            slot_w[n * cap : (n + 1) * cap, :] = weight[0:cap, :]
        for b in range(0, many * cap, exact_rows):
            here = slice(b, b + exact_rows)
            there = batch_rows(batch, b, exact_rows)
            weight = slot_w[here, 0:1]
            total = jnp.zeros((exact_rows, 128), F32)
            for c in range(0, hidden, part_cols):
                span = slice(c, c + part_cols)
                gate = pre_gate[here, span]
                up = pre_up[here, span]
                back = back_proj[here, span]
                sigmoid = 0.5 * jnp.tanh(0.5 * gate) + 0.5
                active = gate * sigmoid
                value = active * up
                product = value * back
                if lane_sums:
                    for lane in range(0, part_cols, 128):
                        total = total + product[:, lane : lane + 128]
                else:
                    row = jnp.sum(product, axis=1, keepdims=True)
                    total = total + jnp.where(first_lane, row, 0.0)
                scaled_ref[there, span] = (weight * value).astype(BF16)
                grad = weight * back
                gate_pre[there, span] = (
                    grad * up * (sigmoid * (1.0 + gate * (1.0 - sigmoid)))
                ).astype(BF16)
                up_pre[there, span] = (grad * active).astype(BF16)
            slot_sum[here, :] = jnp.broadcast_to(
                jnp.sum(total, axis=1, keepdims=True), (exact_rows, 128)
            )
        for n in range(many):
            column = slot_sum[n * cap : (n + 1) * cap, :]
            block_sum = jnp.concatenate([column, jnp.zeros((128 - cap, 128), F32)], axis=0)
            gate_send_ref[first + n] = block_sum.T[0:1, :]

    def slot_grads(back, r, own):
        j, count = batches[back]
        at = group_range(j, count)
        target = lax.rem(y + r, n_y)
        block = cols(target * 2 + (core if own else 1 - core))
        part_ref[at, block] = (
            matmul_nn(gate_pre[at, :], gate_t[:, block]) + matmul_nn(up_pre[at, :], up_t[:, block])
        ).astype(BF16)
        if not own:
            rcore_copy(target, j, count, r, back).start()

    def across_arrives(back):
        for r in range(1, n_y):
            rcore_copy(lax.rem(y + r, n_y), *batches[back], r, back).wait_recv()

    def across(j, i):
        chunk = chunk_at(j, i)
        here = chunk_rows(chunk)
        for r in range(1, n_y):
            target = lax.rem(y + r, n_y)
            mine = part_ref[here, cols(target * 2 + core)].astype(F32)
            y_out[target, here] = (mine + core_buf[target, here].astype(F32)).astype(BF16)
            ry_copy(y, target, chunk, r).start()

    def own_arrives(back):
        rcore_copy(y, *batches[back], 0, back).wait_recv()

    def scatter(j, i):
        chunk = chunk_at(j, i)
        here = chunk_rows(chunk)
        value = part_ref[here, cols(tp)].astype(F32) + core_buf[y, here].astype(F32)
        for r in range(1, n_y):
            source = lax.rem(y + n_y - r, n_y)
            ry_copy(source, y, chunk, r).wait_recv()
            value = value + y_buf[source, here].astype(F32)
        ep_out[here, :] = value.astype(BF16)
        each_source(j, i, lambda dst: rep_copy(dst, ep).start())

    def each(chosen, body):
        for j, i in chosen:
            body(j, i)

    def slots_other(back):
        for r in range(1, n_y):
            slot_grads(back, r, False)
            slot_grads(back, r, True)

    def slots_own(back):
        slot_grads(back, 0, False)
        slot_grads(back, 0, True)

    def prep_tile(source, target, turns):
        def turn(i, carry):
            span = pl.ds(pl.multiple_of(i * block_rows, block_rows), block_rows)
            target[:, span] = source[span, :].T
            return carry

        lax.fori_loop(0, turns, turn, 0)

    block_rows = 256 if features % 256 == 0 else features
    blocks = features // block_rows

    def prep_down():
        for c in range(0, hidden, part_cols):
            down_t[:, c : c + part_cols] = down_w[c : c + part_cols, :].T

    final = len(batches) - 1

    def send_gates():
        loop(1, n_tp, lambda r: tp_copy(lax.rem(tp + r, n_tp), tp).start())
        gate_buf[tp] = gate_send_ref[...]

    def add_gates():
        whole(gate_buf.at[pl.ds(0, n_tp - 1)], recv=2)
        total = gate_buf[0]
        for r in range(1, n_tp):
            total = total + gate_buf[r]
        gate_back_out[...] = total
        loop(1, n_ep, lambda r: gate_copy(lax.rem(ep + r, n_ep), ep).start())
        gate_back[ep] = gate_back_out[ep]

    first = chunks_of(0)
    half = (len(first) + 1) // 2
    each(first[:1], relay)
    for load in loads[4:]:
        load.wait()
    prep_down()
    each(first[1:half], relay)
    prep_tile(gate_w, gate_t, blocks)
    each(first[half:], relay)
    prep_tile(up_w, up_t, blocks)
    near_product(0)
    whole(full_w_ref.at[pl.ds(0, others)], recv=0)
    if final == 2:
        second, third = chunks_of(1), chunks_of(2)
        each(second[:1], relay)
        each(first, forward)
        each(second[1:], relay)
        far_product(0)
        gradients(0)
        slots_other(0)
        each(third[:1], relay)
        each(second, forward)
        near_product(1)
        each(third[1:], relay)
        far_product(1)
        gradients(1)
        slots_other(1)
        slots_own(1)
        across_arrives(1)
        each(second, across)
        near_product(2)
        each(third, forward)
        slots_own(0)
        across_arrives(0)
        each(first[:half], across)
        far_product(2)
        gradients(2)
        send_gates()
        slots_other(2)
        each(first[half:], across)
        own_arrives(1)
        each(second, scatter)
        slots_own(2)
        across_arrives(2)
        each(third, across)
    else:
        for b in range(final + 1):
            if b > 0:
                each(chunks_of(b), relay)
                near_product(b)
            each(chunks_of(b), forward)
            far_product(b)
            gradients(b)
            slots_other(b)
            slots_own(b)
            across_arrives(b)
            each(chunks_of(b), across)
        send_gates()

    tile = 512 if features % 512 == 0 else features
    tiles = features // tile

    def gate_tile(i, carry):
        span = pl.ds(pl.multiple_of(i * tile, tile), tile)
        x = full_ref[0, :, span]
        for row, (grad, out) in enumerate(((gate_pre, gate_res), (up_pre, up_res))):
            total = matmul_tn(x, grad[...])
            out[0, span, :] = total.astype(BF16)
            square = jnp.sum(total * total, axis=1, keepdims=True)
            square_buf[tp, row : row + 1, span] = jnp.broadcast_to(square, (tile, 128)).T[0:1, :]
        return carry

    down_tile = 256 if hidden % 256 == 0 else hidden
    tangents = full_ref.at[1]

    def down_part(i):
        span = slice(i * down_tile, (i + 1) * down_tile)
        total = matmul_tn(scaled_ref[:, span], tangents[...])
        down_res[0, span, :] = total.astype(BF16)
        square = jnp.sum(total * total, axis=1, keepdims=True)
        down_square_out[0:1, span] = jnp.broadcast_to(square, (down_tile, 128)).T[0:1, :] / features

    def tiles_to(first, end):
        lax.fori_loop(min(first, tiles), min(end, tiles), gate_tile, 0)

    tiles_to(0, 1)
    add_gates()
    tiles_to(1, 2)
    for b in range(final):
        if final != 2 or b != 1:
            own_arrives(b)
            each(chunks_of(b), scatter)
    own_arrives(final)
    each(chunks_of(final)[:1], scatter)
    tiles_to(2, 3)
    each(chunks_of(final)[1:], scatter)
    own_back = pltpu.make_async_copy(
        ep_out.at[source_rows(ep)], back_ref.at[source_rows(ep)], own_sem.at[2]
    )
    own_back.start()

    whole(gate_back.at[pl.ds(0, others)], recv=3)
    routes = routes_ref[...]
    weights = weights_ref[...].astype(F32)
    labels = lax.broadcasted_iota(jnp.int32, (n_ep, tok), 0)
    rest = jnp.concatenate([gate_back[e] for e in range(n_ep)], axis=0)
    pieces = []
    for _ in range(3):
        pieces.append(rest.astype(BF16).astype(F32))
        rest = rest - pieces[-1]
    picked = matmul_nt(
        jnp.concatenate(pieces, axis=0).astype(BF16), lane_pick(n_ep, cap).astype(BF16)
    )
    mask = own_block(n_ep, cap)
    spread = (picked * jnp.concatenate([mask] * 3, axis=0)).astype(BF16)
    parts = matmul_nn(spread, table_ref[...])
    values = (parts[0:n_ep] + parts[n_ep : 2 * n_ep]) + parts[2 * n_ep :]
    grads = []
    mixed = jnp.zeros((1, tok), F32)
    for k in range(top):
        same = routes[k : k + 1, :] == labels
        grads.append(jnp.sum(jnp.where(same, values, 0.0), axis=0, keepdims=True))
        gate_out[k : k + 1, :] = grads[k]
        mixed = mixed + weights[k : k + 1, :] * grads[k]
    signal = jnp.zeros((n_ep, tok), F32)
    for k in range(top):
        logit = weights[k : k + 1, :] * (grads[k] - mixed)
        signal = signal + jnp.where(routes[k : k + 1, :] == labels, logit, 0.0)
    signal = signal.astype(BF16)
    term = matmul_nn(signal, tokens_ref[...])
    for e in range(n_ep):
        term_ref[e] = term[e : e + 1, :]
    signal_out[...] = signal
    loop(1, n_ep, lambda r: term_copy(lax.rem(ep + r, n_ep), ep).start())
    term_buf[ep] = term_ref[ep]
    tiles_to(3, tiles)
    loop(1, n_tp, lambda r: square_copy(lax.rem(tp + r, n_tp), tp).start())
    for i in range(hidden // down_tile):
        down_part(i)
    part_slots = pl.ds(0, others * cap)
    whole(slots_ref.at[:, part_slots], send=0)
    whole(full_w_ref.at[pl.ds(0, others)], send=1)
    whole(full_ref.at[:, :, pl.ds(0, (n_y - 1) * width)], send=2)
    whole(full_ref.at[:, :, pl.ds(0, n_y * width)], send=3)
    whole(core_buf, send=4)
    whole(y_out.at[pl.ds(0, n_y - 1)], send=5)
    whole(gate_buf.at[pl.ds(0, n_tp - 1)], send=7)
    whole(gate_back.at[pl.ds(0, others)], send=8)
    whole(square_buf.at[pl.ds(0, n_tp - 1)], send=9)

    own_back.wait()
    whole(back_ref.at[part_slots], recv=1)
    whole(term_buf.at[pl.ds(0, others)], recv=5)
    whole(square_buf.at[pl.ds(0, n_tp - 1)], recv=4)
    whole(back_ref.at[part_slots], send=6)
    whole(term_buf.at[pl.ds(0, others)], send=10)


def batches_of(groups):
    if groups == 4:
        return ((0, 2), (2, 1), (3, 1))
    return tuple((j, 1) for j in range(groups))


def layer(routes, weights, tokens, cotangent, gate, up, down, n_ep, n_tp, cap):
    tok, width = tokens.shape
    features, hidden = gate.shape[1:]
    chunks = n_ep if n_ep <= 8 else next(c for c in range(8, 0, -1) if n_ep % c == 0)
    size = 2 if chunks % 2 == 0 else 1
    n_y = n_tp // 2
    slots = n_ep * cap
    batches = batches_of(chunks // size)
    batch_rows = slots // chunks * size * max(count for _, count in batches)
    dma = pltpu.SemaphoreType.DMA
    in_vmem = pl.BlockSpec(memory_space=VMEM)
    in_hbm = pl.BlockSpec(memory_space=pltpu.HBM)
    return pl.pallas_call(
        functools.partial(layer_kernel, n_ep, n_tp, chunks, cap),
        out_shape=(
            VMEM(gate.shape, BF16),
            VMEM(up.shape, BF16),
            VMEM(down.shape, BF16),
            VMEM((slots, width), BF16),
            VMEM((slots, tok), BF16),
            VMEM((n_ep, tok), BF16),
            VMEM((n_ep, 1, width), F32),
            VMEM((n_tp, 2, features), F32),
            VMEM(routes.shape, F32),
            VMEM((1, hidden), F32),
        ),
        in_specs=[in_hbm] * 7,
        out_specs=[in_vmem] * 10,
        scratch_shapes=[
            VMEM(routes.shape, routes.dtype),
            VMEM(weights.shape, BF16),
            VMEM(tokens.shape, BF16),
            VMEM(tokens.shape, BF16),
            VMEM((features, hidden), BF16),
            VMEM((features, hidden), BF16),
            VMEM((hidden, features), BF16),
            VMEM((hidden, features), BF16),
            VMEM((hidden, features), BF16),
            VMEM((features, hidden), BF16),
            VMEM((2, slots, width), BF16),
            VMEM((n_ep, 1, 128), F32),
            VMEM((2, slots, features), BF16),
            VMEM((n_ep, 1, 128), F32),
            VMEM((batch_rows, hidden), F32),
            VMEM((batch_rows, hidden), F32),
            VMEM((batch_rows, hidden), F32),
            VMEM((batch_rows, 128), F32),
            VMEM((batch_rows, 128), F32),
            VMEM((slots, hidden), BF16),
            VMEM((slots, hidden), BF16),
            VMEM((slots, hidden), BF16),
            VMEM((slots, features), BF16),
            VMEM((n_ep, 1, 128), F32),
            VMEM((n_tp, n_ep, 1, 128), F32),
            VMEM((n_ep, 1, 128), F32),
            VMEM((n_ep, 1, 128), F32),
            VMEM((n_y, slots, width), BF16),
            VMEM((n_y, slots, width), BF16),
            VMEM((n_y, slots, width), BF16),
            VMEM((slots, width), BF16),
            VMEM((n_ep, 1, width), F32),
            dma((7,)),
            dma((3,)),
            dma((11,)),
            dma((6,)),
            dma((2, n_ep)),
            dma((n_y - 1, 2, chunks)),
            dma((n_y, 2, len(batches))),
            dma((n_y, len(batches))),
            dma((n_y - 1, chunks)),
        ],
        compiler_params=pltpu.CompilerParams(
            collective_id=0, has_side_effects=True, vmem_limit_bytes=48 * 2**20
        ),
        name="layer",
    )(routes, weights, tokens, cotangent, gate, up, down)


def finish_kernel(
    hidden,
    gate_ref,
    up_ref,
    down_ref,
    back_ref,
    table_ref,
    signal_ref,
    term_buf,
    square_buf,
    gate_grad_ref,
    down_square_ref,
    router_hbm,
    gate_out,
    up_out,
    down_out,
    token_out,
    gate_grad_out,
    term_out,
    gate_square_out,
    up_square_out,
    down_square_out,
    router_ref,
    token_ref,
    term_ref,
    gate_square_ref,
    up_square_ref,
    sems,
):
    tp = lax.axis_index("tp")
    n_ep, _, width = term_buf.shape
    load = pltpu.make_async_copy(router_hbm, router_ref, sems.at[0])
    load.start()
    pairs = (
        (gate_ref, gate_out),
        (up_ref, up_out),
        (down_ref, down_out),
        (gate_grad_ref, gate_grad_out),
        (down_square_ref, down_square_out),
        (term_ref, term_out),
        (gate_square_ref, gate_square_out),
        (up_square_ref, up_square_out),
        (token_ref, token_out),
    )
    copies = [pltpu.make_async_copy(*pair, sems.at[i + 1]) for i, pair in enumerate(pairs)]
    for copy in copies[:5]:
        copy.start()
    term = term_buf[0]
    for e in range(1, n_ep):
        term = term + term_buf[e]
    term_ref[...] = term
    square = square_buf[0]
    for r in range(1, square_buf.shape[0]):
        square = square + square_buf[r]
    square = square / hidden
    gate_square_ref[...] = square[0:1, :]
    up_square_ref[...] = square[1:2, :]
    for copy in copies[5:8]:
        copy.start()
    token = matmul_tn(table_ref[...], back_ref[...])
    load.wait()
    cols = pl.ds(pl.multiple_of(tp * width, width), width)
    token_ref[...] = token + matmul_tn(signal_ref[...], router_ref[:, cols])
    copies[8].start()
    for copy in copies:
        copy.wait()


def finish(results, router_rows, hidden):
    gates, ups, downs, back, _, _, terms, squares, gate_grad, down_square = results
    tok, width = gate_grad.shape[1], back.shape[1]
    features = squares.shape[2]
    outs = (
        (gates.shape, BF16),
        (ups.shape, BF16),
        (downs.shape, BF16),
        ((tok, width), F32),
        (gate_grad.shape, F32),
        (terms.shape[1:], F32),
        ((1, features), F32),
        ((1, features), F32),
        (down_square.shape, F32),
    )
    count = len(results)
    return pl.pallas_call(
        functools.partial(finish_kernel, hidden),
        out_shape=tuple(jax.ShapeDtypeStruct(*out) for out in outs),
        in_specs=[pl.BlockSpec(memory_space=VMEM)] * count + [pl.BlockSpec(memory_space=pltpu.HBM)],
        out_specs=[pl.BlockSpec(memory_space=pltpu.HBM)] * len(outs),
        scratch_shapes=[
            VMEM(router_rows.shape, BF16),
            VMEM((tok, width), F32),
            VMEM((1, width), F32),
            VMEM((1, features), F32),
            VMEM((1, features), F32),
            pltpu.SemaphoreType.DMA((10,)),
        ],
        compiler_params=pltpu.CompilerParams(vmem_limit_bytes=4 * 2**20),
        name="finish",
    )(*(pltpu.with_memory_space_constraint(a, VMEM) for a in results), router_rows)


def shards(tokens, routing, gate_weights, cotangent, expert_gate, expert_up, expert_down, router):
    tok_rows = tokens.shape[0]
    top_count = routing.shape[1]
    experts = router.shape[1]
    n_tp = lax.axis_size("tp")
    n_ep = lax.axis_size("ep")
    capacity = 3 * top_count * tok_rows // (2 * experts)
    results = layer(
        routing.T,
        gate_weights.T,
        tokens,
        cotangent,
        expert_gate,
        expert_up,
        expert_down,
        n_ep,
        n_tp,
        capacity,
    )
    hidden = expert_gate.shape[2] * n_tp
    gates, ups, downs, token_grad, gate_grad, router_grad, gate_square, up_square, down_square = (
        finish(results, router.T, hidden)
    )
    return (
        token_grad,
        gate_grad.T,
        gates,
        ups,
        downs,
        router_grad,
        gate_square,
        up_square,
        down_square,
    )


def solution(mesh):
    in_specs = (
        P("ep", "tp"),
        P("ep", None),
        P("ep", None),
        P("ep", "tp"),
        P("ep", None, "tp"),
        P("ep", None, "tp"),
        P("ep", "tp", None),
        P(),
    )
    out_specs = (
        P("ep", "tp"),
        P("ep", None),
        P("ep", None, "tp"),
        P("ep", None, "tp"),
        P("ep", "tp", None),
        P("ep", "tp"),
        P("ep", None),
        P("ep", None),
        P("ep", "tp"),
    )
    return jax.shard_map(shards, mesh=mesh, in_specs=in_specs, out_specs=out_specs, check_vma=False)
```

```python
import functools

import jax
import jax.numpy as jnp
from jax import lax
from jax.experimental import pallas as pl
from jax.experimental.pallas import tpu as pltpu
from jax.sharding import PartitionSpec as P

MESH = pl.DeviceIdType.MESH
F32 = jnp.float32
BF16 = jnp.bfloat16
VMEM = pltpu.VMEM


def matmul_nn(left_side, right_side):
    return jnp.dot(left_side, right_side, preferred_element_type=F32)


def matmul_tn(left_side, right_side):
    return lax.dot_general(
        left_side, right_side, (((0,), (0,)), ((), ())), preferred_element_type=F32
    )


def matmul_nt(left_side, right_side):
    return lax.dot_general(
        left_side, right_side, (((1,), (1,)), ((), ())), preferred_element_type=F32
    )


def loop(lower, upper, body):
    if upper - lower <= 8:
        for i in range(lower, upper):
            body(i)
    else:
        lax.fori_loop(lower, upper, lambda i, carry: (body(i), carry)[1], 0)


def place():
    ep, tp = lax.axis_index("ep"), lax.axis_index("tp")
    return ep, tp, lax.div(tp, 2), lax.rem(tp, 2)


def paired(value, step, count):
    if count & (count - 1):
        return lax.rem(value + step, count)
    out, bit = value, 1
    while bit < count:
        asked = lax.rem(lax.div(jnp.int32(step), bit), 2)
        out = out + asked * bit * (1 - 2 * lax.rem(lax.div(value, bit), 2))
        bit *= 2
    return out


def greet(n_ep, n_tp, between=None):
    ep, tp, _, _ = place()
    barrier = pltpu.get_barrier_semaphore()

    def to_ep(r):
        pl.semaphore_signal(
            barrier, inc=1, device_id=(lax.rem(ep + r, n_ep), tp), device_id_type=MESH
        )

    def to_tp(r):
        pl.semaphore_signal(
            barrier, inc=1, device_id=(ep, lax.rem(tp + r, n_tp)), device_id_type=MESH
        )

    loop(1, n_ep, to_ep)
    loop(1, n_tp, to_tp)
    if between is not None:
        between()
    pl.semaphore_wait(barrier, n_ep - 1 + n_tp - 1)


def lane_pick(n_ep, cap):
    shape = (n_ep, cap, 128)
    pick = lax.broadcasted_iota(jnp.int32, shape, 1) == lax.broadcasted_iota(jnp.int32, shape, 2)
    return pick.astype(F32).reshape(n_ep * cap, 128)


def own_block(n_ep, cap):
    shape = (n_ep, n_ep * cap)
    first = lax.broadcasted_iota(jnp.int32, shape, 0) * cap
    slot = lax.broadcasted_iota(jnp.int32, shape, 1)
    return ((slot >= first) & (slot < first + cap)).astype(F32)


def fill_slots(cap, routes_ref, weights_ref, tokens_ref, cotangent_ref, table_ref, out_ref, w_ref):
    n_ep = w_ref.shape[0]
    width = out_ref.shape[2]
    top, tok = routes_ref.shape
    routes = routes_ref[...]
    weights = weights_ref[...].astype(F32)
    labels = lax.broadcasted_iota(jnp.int32, (n_ep, tok), 0)
    hit = jnp.zeros((n_ep, tok), F32)
    chosen = jnp.zeros((n_ep, tok), F32)
    for k in range(top):
        same = routes[k : k + 1, :] == labels
        hit = hit + same.astype(F32)
        chosen = chosen + jnp.where(same, weights[k : k + 1, :], 0.0)
    square = (tok, tok)
    before = lax.broadcasted_iota(jnp.int32, square, 0) < lax.broadcasted_iota(jnp.int32, square, 1)
    count = matmul_nn(hit.astype(BF16), before.astype(F32).astype(BF16))
    position = jnp.where(hit > 0.0, count, -1.0)
    slot = lax.broadcasted_iota(jnp.int32, (n_ep, cap, tok), 1).astype(F32)
    table = (slot == position[:, None, :]).astype(F32).reshape(n_ep * cap, tok).astype(BF16)
    table_ref[...] = table
    for which, source in enumerate((tokens_ref, cotangent_ref)):
        out_ref[which] = matmul_nn(table, source[...]).astype(BF16)
    spread = matmul_nt(chosen.astype(BF16), table) * own_block(n_ep, cap)
    values = matmul_nn(spread.astype(BF16), lane_pick(n_ep, cap).astype(BF16))
    for e in range(n_ep):
        w_ref[e] = values[e : e + 1, :]


def layer_kernel(
    n_ep,
    n_tp,
    chunks,
    cap,
    routes_hbm,
    weights_hbm,
    tokens_hbm,
    cotangent_hbm,
    gate_hbm,
    up_hbm,
    down_hbm,
    gate_res,
    up_res,
    down_res,
    back_ref,
    table_ref,
    signal_out,
    term_buf,
    square_buf,
    gate_out,
    down_square_out,
    routes_ref,
    weights_ref,
    tokens_ref,
    cotangent_ref,
    gate_w,
    up_w,
    down_w,
    gate_t,
    up_t,
    down_t,
    slots_ref,
    w_ref,
    full_ref,
    full_w_ref,
    pre_gate,
    pre_up,
    back_proj,
    slot_w,
    slot_sum,
    scaled_ref,
    gate_pre,
    up_pre,
    part_ref,
    gate_send_ref,
    gate_buf,
    gate_back_out,
    gate_back,
    core_buf,
    y_out,
    y_buf,
    ep_out,
    term_ref,
    load_sem,
    own_sem,
    send_sem,
    all_recv,
    ep_recv,
    y_recv,
    core_recv,
    rcore_recv,
    ry_recv,
):
    ep, tp, y, core = place()
    n_y = n_tp // 2
    partner = y * 2 + 1 - core
    slots, features = part_ref.shape
    width = features // n_tp
    hidden = gate_w.shape[1]
    top, tok = routes_ref.shape
    per = n_ep // chunks
    rows = per * cap
    size = 2 if chunks % 2 == 0 else 1
    groups = chunks // size
    group_rows = size * rows
    exact_rows = 16 if group_rows % 16 == 0 else 8

    batches = batches_of(groups)

    def cols(which):
        return pl.ds(pl.multiple_of(which * width, width), width)

    def y_cols(which):
        return pl.ds(pl.multiple_of(which * (2 * width), 2 * width), 2 * width)

    def base_of(j, count):
        return lax.div(group_at(j), count) * count

    def group_range(j, count, start=0, many=None):
        first = base_of(j, count) * group_rows + start
        return pl.ds(
            pl.multiple_of(first, exact_rows), count * group_rows if many is None else many
        )

    def batch_rows(batch, start=0, many=None):
        return group_range(*batches[batch], start, many)

    def chunk_rows(chunk):
        return pl.ds(pl.multiple_of(chunk * rows, rows), rows)

    def source_rows(source):
        return pl.ds(pl.multiple_of(source * cap, cap), cap)

    def remote(src, dst, send, recv, device):
        return pltpu.make_async_remote_copy(
            src_ref=src,
            dst_ref=dst,
            send_sem=send,
            recv_sem=recv,
            device_id=device,
            device_id_type=MESH,
        )

    def group_at(j):
        return paired(lax.div(ep, per * size), j, groups)

    def chunk_at(j, i):
        return group_at(j) * size + paired(lax.rem(lax.div(ep, per), size), i, size)

    def ep_copy(dst, src, part):
        return remote(
            slots_ref.at[part, source_rows(dst), :],
            full_ref.at[part, source_rows(src), cols(tp)],
            send_sem.at[0],
            ep_recv.at[part, src],
            (dst, tp),
        )

    def w_copy(dst, src):
        return remote(w_ref.at[dst], full_w_ref.at[src], send_sem.at[1], all_recv.at[0], (dst, tp))

    def y_copy(source_y, target_y, at, slot, r, part):
        piece = full_ref.at[part, at, cols(source_y * 2 + core)]
        return remote(
            piece, piece, send_sem.at[2], y_recv.at[r - 1, part, slot], (ep, target_y * 2 + core)
        )

    def core_copy(source_y, source_core, at, slot, batch, part):
        piece = full_ref.at[part, at, cols(source_y * 2 + source_core)]
        return remote(piece, piece, send_sem.at[3], core_recv.at[slot, part, batch], (ep, partner))

    def rcore_copy(target_y, j, count, slot, back):
        at = group_range(j, count)
        return remote(
            part_ref.at[at, cols(target_y * 2 + 1 - core)],
            core_buf.at[target_y, at],
            send_sem.at[4],
            rcore_recv.at[slot, back],
            (ep, partner),
        )

    def ry_copy(source_y, target_y, chunk, r):
        return remote(
            y_out.at[target_y, chunk_rows(chunk)],
            y_buf.at[source_y, chunk_rows(chunk)],
            send_sem.at[5],
            ry_recv.at[r - 1, chunk],
            (ep, target_y * 2 + core),
        )

    def rep_copy(dst, src):
        return remote(
            ep_out.at[source_rows(dst)],
            back_ref.at[source_rows(src)],
            send_sem.at[6],
            all_recv.at[1],
            (dst, tp),
        )

    def tp_copy(dst, src):
        return remote(
            gate_send_ref, gate_buf.at[src], send_sem.at[7], all_recv.at[2], (ep, dst)
        )

    def gate_copy(dst, src):
        return remote(
            gate_back_out.at[dst], gate_back.at[src], send_sem.at[8], all_recv.at[3], (dst, tp)
        )

    def square_copy(dst, src):
        return remote(
            square_buf.at[src], square_buf.at[src], send_sem.at[9], all_recv.at[4], (ep, dst)
        )

    def term_copy(dst, src):
        return remote(
            term_ref.at[dst], term_buf.at[src], send_sem.at[10], all_recv.at[5], (dst, tp)
        )

    def whole(ref, send=None, recv=None):
        copy = remote(
            ref,
            ref,
            send_sem.at[0 if send is None else send],
            all_recv.at[0 if recv is None else recv],
            (ep, partner),
        )
        if send is not None:
            copy.wait_send()
        if recv is not None:
            copy.wait_recv()

    others = n_ep - 1

    pairs = (
        (routes_hbm, routes_ref),
        (weights_hbm, weights_ref),
        (tokens_hbm, tokens_ref),
        (cotangent_hbm, cotangent_ref),
        (gate_hbm.at[0], gate_w),
        (up_hbm.at[0], up_w),
        (down_hbm.at[0], down_w),
    )
    loads = [pltpu.make_async_copy(*pair, load_sem.at[i]) for i, pair in enumerate(pairs)]

    def begin():
        for load in loads:
            load.start()
        for load in loads[:4]:
            load.wait()
        fill()

    fill = functools.partial(
        fill_slots,
        cap,
        routes_ref,
        weights_ref,
        tokens_ref,
        cotangent_ref,
        table_ref,
        slots_ref,
        w_ref,
    )
    greet(n_ep, n_tp, begin)

    own_rows = pltpu.make_async_copy(
        slots_ref.at[:, source_rows(ep), :],
        full_ref.at[:, source_rows(ep), cols(tp)],
        own_sem.at[0],
    )
    own_w = pltpu.make_async_copy(w_ref.at[ep], full_w_ref.at[ep], own_sem.at[1])
    own_rows.start()
    own_w.start()

    def each_source(j, i, body):
        chunk = chunk_at(j, i)

        def one(n):
            source = chunk * per + n

            @pl.when(source != ep)
            def _():
                body(source)

        loop(0, per, one)

    def send_group(j):
        for i in range(size):
            for part in range(2):
                each_source(j, i, lambda dst: ep_copy(dst, ep, part).start())

    loop(1, n_ep, lambda r: w_copy(lax.rem(ep + r, n_ep), ep).start())
    loop(0, groups, send_group)
    gate_send_ref[...] = jnp.zeros_like(gate_send_ref)
    own_rows.wait()
    own_w.wait()

    def batch_of(j):
        return next(b for b, (k, count) in enumerate(batches) if k <= j < k + count)

    def y_slot(j, i):
        return max(0, (j - batches[0][1]) * size + i + 1) if j >= batches[0][1] else 0

    def relay(j, i):
        chunk = chunk_at(j, i)
        for part in range(2):
            each_source(j, i, lambda source: ep_copy(ep, source, part).wait_recv())
            for r in range(1, n_y):
                at = chunk_rows(chunk)
                y_copy(y, lax.rem(y + r, n_y), at, y_slot(j, i), r, part).start()
            core_copy(y, core, chunk_rows(chunk), 0, batch_of(j), part).start()

    def forward(j, i):
        chunk = chunk_at(j, i)
        for part in range(2):
            for r in range(1, n_y):
                source_y = lax.rem(y + n_y - r, n_y)
                at = chunk_rows(chunk)
                y_copy(source_y, y, at, y_slot(j, i), r, part).wait_recv()
                core_copy(source_y, core, at, r, batch_of(j), part).start()

    def forward_first():
        at = batch_rows(0)
        for part in range(2):
            for r in range(1, n_y):
                source_y = lax.rem(y + n_y - r, n_y)
                y_copy(source_y, y, at, 0, r, part).wait_recv()
                core_copy(source_y, core, at, r, 0, part).start()

    def chunks_of(batch):
        j, count = batches[batch]
        return [(k, i) for k in range(j, j + count) for i in range(size)]

    def product(batch, source_y, slot):
        at = batch_rows(batch)
        many = batches[batch][1] * group_rows
        k = y_cols(source_y)

        def put(out, value):
            out[0:many, :] = value if slot == 0 else out[0:many, :] + value

        core_copy(source_y, 1 - core, at, slot, batch, 0).wait_recv()
        put(pre_gate, matmul_nn(full_ref[0, at, k], gate_w[k, :]))
        put(pre_up, matmul_nn(full_ref[0, at, k], up_w[k, :]))
        core_copy(source_y, 1 - core, at, slot, batch, 1).wait_recv()
        put(back_proj, matmul_nn(full_ref[1, at, k], down_t[k, :]))

    def near_product(batch):
        product(batch, y, 0)

    def far_product(batch):
        for r in range(1, n_y):
            product(batch, lax.rem(y + n_y - r, n_y), r)

    part_cols = 256 if hidden % 256 == 0 else hidden
    lane_sums = part_cols % 128 == 0
    first_lane = lax.broadcasted_iota(jnp.int32, (exact_rows, 128), 1) == 0

    def gradients(batch):
        first = base_of(*batches[batch]) * (size * per)
        many = batches[batch][1] * size * per
        for n in range(many):
            weight = jnp.broadcast_to(full_w_ref[first + n], (128, 128)).T
            slot_w[n * cap : (n + 1) * cap, :] = weight[0:cap, :]
        for b in range(0, many * cap, exact_rows):
            here = slice(b, b + exact_rows)
            there = batch_rows(batch, b, exact_rows)
            weight = slot_w[here, 0:1]
            total = jnp.zeros((exact_rows, 128), F32)
            for c in range(0, hidden, part_cols):
                span = slice(c, c + part_cols)
                gate = pre_gate[here, span]
                up = pre_up[here, span]
                back = back_proj[here, span]
                sigmoid = 0.5 * jnp.tanh(0.5 * gate) + 0.5
                active = gate * sigmoid
                value = active * up
                product = value * back
                if lane_sums:
                    for lane in range(0, part_cols, 128):
                        total = total + product[:, lane : lane + 128]
                else:
                    row = jnp.sum(product, axis=1, keepdims=True)
                    total = total + jnp.where(first_lane, row, 0.0)
                scaled_ref[there, span] = (weight * value).astype(BF16)
                grad = weight * back
                gate_pre[there, span] = (
                    grad * up * (sigmoid * (1.0 + gate * (1.0 - sigmoid)))
                ).astype(BF16)
                up_pre[there, span] = (grad * active).astype(BF16)
            slot_sum[here, :] = jnp.broadcast_to(
                jnp.sum(total, axis=1, keepdims=True), (exact_rows, 128)
            )
        for n in range(many):
            column = slot_sum[n * cap : (n + 1) * cap, :]
            block_sum = jnp.concatenate([column, jnp.zeros((128 - cap, 128), F32)], axis=0)
            gate_send_ref[first + n] = block_sum.T[0:1, :]

    def slot_grads(back, r, own):
        j, count = batches[back]
        at = group_range(j, count)
        target = lax.rem(y + r, n_y)
        block = cols(target * 2 + (core if own else 1 - core))
        part_ref[at, block] = (
            matmul_nn(gate_pre[at, :], gate_t[:, block]) + matmul_nn(up_pre[at, :], up_t[:, block])
        ).astype(BF16)
        if not own:
            rcore_copy(target, j, count, r, back).start()

    def across_arrives(back):
        for r in range(1, n_y):
            rcore_copy(lax.rem(y + r, n_y), *batches[back], r, back).wait_recv()

    def across(j, i):
        chunk = chunk_at(j, i)
        here = chunk_rows(chunk)
        for r in range(1, n_y):
            target = lax.rem(y + r, n_y)
            mine = part_ref[here, cols(target * 2 + core)].astype(F32)
            y_out[target, here] = (mine + core_buf[target, here].astype(F32)).astype(BF16)
            ry_copy(y, target, chunk, r).start()

    def own_arrives(back):
        rcore_copy(y, *batches[back], 0, back).wait_recv()

    def scatter(j, i):
        chunk = chunk_at(j, i)
        here = chunk_rows(chunk)
        value = part_ref[here, cols(tp)].astype(F32) + core_buf[y, here].astype(F32)
        for r in range(1, n_y):
            source = lax.rem(y + n_y - r, n_y)
            ry_copy(source, y, chunk, r).wait_recv()
            value = value + y_buf[source, here].astype(F32)
        ep_out[here, :] = value.astype(BF16)
        each_source(j, i, lambda dst: rep_copy(dst, ep).start())

    def each(chosen, body):
        for j, i in chosen:
            body(j, i)

    def slots_other(back):
        for r in range(1, n_y):
            slot_grads(back, r, False)
            slot_grads(back, r, True)

    def slots_own(back):
        slot_grads(back, 0, False)
        slot_grads(back, 0, True)

    def prep_tile(source, target, turns):
        def turn(i, carry):
            span = pl.ds(pl.multiple_of(i * block_rows, block_rows), block_rows)
            target[:, span] = source[span, :].T
            return carry

        lax.fori_loop(0, turns, turn, 0)

    block_rows = 256 if features % 256 == 0 else features
    blocks = features // block_rows

    def prep_down():
        for c in range(0, hidden, part_cols):
            down_t[:, c : c + part_cols] = down_w[c : c + part_cols, :].T

    final = len(batches) - 1

    def send_gates():
        loop(1, n_tp, lambda r: tp_copy(lax.rem(tp + r, n_tp), tp).start())
        gate_buf[tp] = gate_send_ref[...]

    def add_gates():
        whole(gate_buf.at[pl.ds(0, n_tp - 1)], recv=2)
        total = gate_buf[0]
        for r in range(1, n_tp):
            total = total + gate_buf[r]
        gate_back_out[...] = total
        loop(1, n_ep, lambda r: gate_copy(lax.rem(ep + r, n_ep), ep).start())
        gate_back[ep] = gate_back_out[ep]

    first = chunks_of(0)
    half = (len(first) + 1) // 2
    each(first[:1], relay)
    for load in loads[4:]:
        load.wait()
    prep_down()
    each(first[1:half], relay)
    prep_tile(gate_w, gate_t, blocks)
    each(first[half:], relay)
    prep_tile(up_w, up_t, blocks)
    near_product(0)
    whole(full_w_ref.at[pl.ds(0, others)], recv=0)
    if final == 2:
        second, third = chunks_of(1), chunks_of(2)
        each(second[:1], relay)
        forward_first()
        each(second[1:], relay)
        far_product(0)
        gradients(0)
        slots_other(0)
        each(third[:1], relay)
        each(second, forward)
        near_product(1)
        each(third[1:], relay)
        far_product(1)
        gradients(1)
        slots_other(1)
        slots_own(1)
        across_arrives(1)
        each(second, across)
        near_product(2)
        each(third, forward)
        slots_own(0)
        across_arrives(0)
        each(first[:half], across)
        far_product(2)
        gradients(2)
        send_gates()
        slots_other(2)
        each(first[half:], across)
        own_arrives(1)
        each(second, scatter)
        slots_own(2)
        across_arrives(2)
        each(third, across)
    else:
        for b in range(final + 1):
            if b > 0:
                each(chunks_of(b), relay)
                near_product(b)
            if b == 0:
                forward_first()
            else:
                each(chunks_of(b), forward)
            far_product(b)
            gradients(b)
            slots_other(b)
            slots_own(b)
            across_arrives(b)
            each(chunks_of(b), across)
        send_gates()

    tile = 512 if features % 512 == 0 else features
    tiles = features // tile

    def gate_tile(i, carry):
        span = pl.ds(pl.multiple_of(i * tile, tile), tile)
        x = full_ref[0, :, span]
        for row, (grad, out) in enumerate(((gate_pre, gate_res), (up_pre, up_res))):
            total = matmul_tn(x, grad[...])
            out[0, span, :] = total.astype(BF16)
            square = jnp.sum(total * total, axis=1, keepdims=True)
            square_buf[tp, row : row + 1, span] = jnp.broadcast_to(square, (tile, 128)).T[0:1, :]
        return carry

    down_tile = 256 if hidden % 256 == 0 else hidden
    tangents = full_ref.at[1]

    def down_part(i):
        span = slice(i * down_tile, (i + 1) * down_tile)
        total = matmul_tn(scaled_ref[:, span], tangents[...])
        down_res[0, span, :] = total.astype(BF16)
        square = jnp.sum(total * total, axis=1, keepdims=True)
        down_square_out[0:1, span] = jnp.broadcast_to(square, (down_tile, 128)).T[0:1, :] / features

    def tiles_to(first, end):
        lax.fori_loop(min(first, tiles), min(end, tiles), gate_tile, 0)

    tiles_to(0, 1)
    add_gates()
    tiles_to(1, 2)
    for b in range(final):
        if final != 2 or b != 1:
            own_arrives(b)
            each(chunks_of(b), scatter)
    own_arrives(final)
    each(chunks_of(final)[:1], scatter)
    tiles_to(2, 3)
    each(chunks_of(final)[1:], scatter)
    own_back = pltpu.make_async_copy(
        ep_out.at[source_rows(ep)], back_ref.at[source_rows(ep)], own_sem.at[2]
    )
    own_back.start()

    whole(gate_back.at[pl.ds(0, others)], recv=3)
    routes = routes_ref[...]
    weights = weights_ref[...].astype(F32)
    labels = lax.broadcasted_iota(jnp.int32, (n_ep, tok), 0)
    rest = jnp.concatenate([gate_back[e] for e in range(n_ep)], axis=0)
    pieces = []
    for _ in range(3):
        pieces.append(rest.astype(BF16).astype(F32))
        rest = rest - pieces[-1]
    picked = matmul_nt(
        jnp.concatenate(pieces, axis=0).astype(BF16), lane_pick(n_ep, cap).astype(BF16)
    )
    mask = own_block(n_ep, cap)
    spread = (picked * jnp.concatenate([mask] * 3, axis=0)).astype(BF16)
    parts = matmul_nn(spread, table_ref[...])
    values = (parts[0:n_ep] + parts[n_ep : 2 * n_ep]) + parts[2 * n_ep :]
    grads = []
    mixed = jnp.zeros((1, tok), F32)
    for k in range(top):
        same = routes[k : k + 1, :] == labels
        grads.append(jnp.sum(jnp.where(same, values, 0.0), axis=0, keepdims=True))
        gate_out[k : k + 1, :] = grads[k]
        mixed = mixed + weights[k : k + 1, :] * grads[k]
    signal = jnp.zeros((n_ep, tok), F32)
    for k in range(top):
        logit = weights[k : k + 1, :] * (grads[k] - mixed)
        signal = signal + jnp.where(routes[k : k + 1, :] == labels, logit, 0.0)
    signal = signal.astype(BF16)
    term = matmul_nn(signal, tokens_ref[...])
    for e in range(n_ep):
        term_ref[e] = term[e : e + 1, :]
    signal_out[...] = signal
    loop(1, n_ep, lambda r: term_copy(lax.rem(ep + r, n_ep), ep).start())
    term_buf[ep] = term_ref[ep]
    tiles_to(3, tiles)
    loop(1, n_tp, lambda r: square_copy(lax.rem(tp + r, n_tp), tp).start())
    for i in range(hidden // down_tile):
        down_part(i)
    part_slots = pl.ds(0, others * cap)
    whole(slots_ref.at[:, part_slots], send=0)
    whole(full_w_ref.at[pl.ds(0, others)], send=1)
    whole(full_ref.at[:, :, pl.ds(0, (n_y - 1) * width)], send=2)
    whole(full_ref.at[:, :, pl.ds(0, n_y * width)], send=3)
    whole(core_buf, send=4)
    whole(y_out.at[pl.ds(0, n_y - 1)], send=5)
    whole(gate_buf.at[pl.ds(0, n_tp - 1)], send=7)
    whole(gate_back.at[pl.ds(0, others)], send=8)
    whole(square_buf.at[pl.ds(0, n_tp - 1)], send=9)

    own_back.wait()
    whole(back_ref.at[part_slots], recv=1)
    whole(term_buf.at[pl.ds(0, others)], recv=5)
    whole(square_buf.at[pl.ds(0, n_tp - 1)], recv=4)
    whole(back_ref.at[part_slots], send=6)
    whole(term_buf.at[pl.ds(0, others)], send=10)


def batches_of(groups):
    if groups == 4:
        return ((0, 2), (2, 1), (3, 1))
    return tuple((j, 1) for j in range(groups))


def layer(routes, weights, tokens, cotangent, gate, up, down, n_ep, n_tp, cap):
    tok, width = tokens.shape
    features, hidden = gate.shape[1:]
    chunks = n_ep if n_ep <= 8 else next(c for c in range(8, 0, -1) if n_ep % c == 0)
    size = 2 if chunks % 2 == 0 else 1
    n_y = n_tp // 2
    slots = n_ep * cap
    batches = batches_of(chunks // size)
    batch_rows = slots // chunks * size * max(count for _, count in batches)
    dma = pltpu.SemaphoreType.DMA
    in_vmem = pl.BlockSpec(memory_space=VMEM)
    in_hbm = pl.BlockSpec(memory_space=pltpu.HBM)
    return pl.pallas_call(
        functools.partial(layer_kernel, n_ep, n_tp, chunks, cap),
        out_shape=(
            VMEM(gate.shape, BF16),
            VMEM(up.shape, BF16),
            VMEM(down.shape, BF16),
            VMEM((slots, width), BF16),
            VMEM((slots, tok), BF16),
            VMEM((n_ep, tok), BF16),
            VMEM((n_ep, 1, width), F32),
            VMEM((n_tp, 2, features), F32),
            VMEM(routes.shape, F32),
            VMEM((1, hidden), F32),
        ),
        in_specs=[in_hbm] * 7,
        out_specs=[in_vmem] * 10,
        scratch_shapes=[
            VMEM(routes.shape, routes.dtype),
            VMEM(weights.shape, BF16),
            VMEM(tokens.shape, BF16),
            VMEM(tokens.shape, BF16),
            VMEM((features, hidden), BF16),
            VMEM((features, hidden), BF16),
            VMEM((hidden, features), BF16),
            VMEM((hidden, features), BF16),
            VMEM((hidden, features), BF16),
            VMEM((features, hidden), BF16),
            VMEM((2, slots, width), BF16),
            VMEM((n_ep, 1, 128), F32),
            VMEM((2, slots, features), BF16),
            VMEM((n_ep, 1, 128), F32),
            VMEM((batch_rows, hidden), F32),
            VMEM((batch_rows, hidden), F32),
            VMEM((batch_rows, hidden), F32),
            VMEM((batch_rows, 128), F32),
            VMEM((batch_rows, 128), F32),
            VMEM((slots, hidden), BF16),
            VMEM((slots, hidden), BF16),
            VMEM((slots, hidden), BF16),
            VMEM((slots, features), BF16),
            VMEM((n_ep, 1, 128), F32),
            VMEM((n_tp, n_ep, 1, 128), F32),
            VMEM((n_ep, 1, 128), F32),
            VMEM((n_ep, 1, 128), F32),
            VMEM((n_y, slots, width), BF16),
            VMEM((n_y, slots, width), BF16),
            VMEM((n_y, slots, width), BF16),
            VMEM((slots, width), BF16),
            VMEM((n_ep, 1, width), F32),
            dma((7,)),
            dma((3,)),
            dma((11,)),
            dma((6,)),
            dma((2, n_ep)),
            dma((n_y - 1, 2, chunks - batches[0][1] * size + 1)),
            dma((n_y, 2, len(batches))),
            dma((n_y, len(batches))),
            dma((n_y - 1, chunks)),
        ],
        compiler_params=pltpu.CompilerParams(
            collective_id=0, has_side_effects=True, vmem_limit_bytes=48 * 2**20
        ),
        name="layer",
    )(routes, weights, tokens, cotangent, gate, up, down)


def finish_kernel(
    hidden,
    gate_ref,
    up_ref,
    down_ref,
    back_ref,
    table_ref,
    signal_ref,
    term_buf,
    square_buf,
    gate_grad_ref,
    down_square_ref,
    router_hbm,
    gate_out,
    up_out,
    down_out,
    token_out,
    gate_grad_out,
    term_out,
    gate_square_out,
    up_square_out,
    down_square_out,
    router_ref,
    token_ref,
    term_ref,
    gate_square_ref,
    up_square_ref,
    sems,
):
    tp = lax.axis_index("tp")
    n_ep, _, width = term_buf.shape
    load = pltpu.make_async_copy(router_hbm, router_ref, sems.at[0])
    load.start()
    pairs = (
        (gate_ref, gate_out),
        (up_ref, up_out),
        (down_ref, down_out),
        (gate_grad_ref, gate_grad_out),
        (down_square_ref, down_square_out),
        (term_ref, term_out),
        (gate_square_ref, gate_square_out),
        (up_square_ref, up_square_out),
        (token_ref, token_out),
    )
    copies = [pltpu.make_async_copy(*pair, sems.at[i + 1]) for i, pair in enumerate(pairs)]
    for copy in copies[:5]:
        copy.start()
    term = term_buf[0]
    for e in range(1, n_ep):
        term = term + term_buf[e]
    term_ref[...] = term
    square = square_buf[0]
    for r in range(1, square_buf.shape[0]):
        square = square + square_buf[r]
    square = square / hidden
    gate_square_ref[...] = square[0:1, :]
    up_square_ref[...] = square[1:2, :]
    for copy in copies[5:8]:
        copy.start()
    token = matmul_tn(table_ref[...], back_ref[...])
    load.wait()
    cols = pl.ds(pl.multiple_of(tp * width, width), width)
    token_ref[...] = token + matmul_tn(signal_ref[...], router_ref[:, cols])
    copies[8].start()
    for copy in copies:
        copy.wait()


def finish(results, router_rows, hidden):
    gates, ups, downs, back, _, _, terms, squares, gate_grad, down_square = results
    tok, width = gate_grad.shape[1], back.shape[1]
    features = squares.shape[2]
    outs = (
        (gates.shape, BF16),
        (ups.shape, BF16),
        (downs.shape, BF16),
        ((tok, width), F32),
        (gate_grad.shape, F32),
        (terms.shape[1:], F32),
        ((1, features), F32),
        ((1, features), F32),
        (down_square.shape, F32),
    )
    count = len(results)
    return pl.pallas_call(
        functools.partial(finish_kernel, hidden),
        out_shape=tuple(jax.ShapeDtypeStruct(*out) for out in outs),
        in_specs=[pl.BlockSpec(memory_space=VMEM)] * count + [pl.BlockSpec(memory_space=pltpu.HBM)],
        out_specs=[pl.BlockSpec(memory_space=pltpu.HBM)] * len(outs),
        scratch_shapes=[
            VMEM(router_rows.shape, BF16),
            VMEM((tok, width), F32),
            VMEM((1, width), F32),
            VMEM((1, features), F32),
            VMEM((1, features), F32),
            pltpu.SemaphoreType.DMA((10,)),
        ],
        compiler_params=pltpu.CompilerParams(vmem_limit_bytes=4 * 2**20),
        name="finish",
    )(*(pltpu.with_memory_space_constraint(a, VMEM) for a in results), router_rows)


def shards(tokens, routing, gate_weights, cotangent, expert_gate, expert_up, expert_down, router):
    tok_rows = tokens.shape[0]
    top_count = routing.shape[1]
    experts = router.shape[1]
    n_tp = lax.axis_size("tp")
    n_ep = lax.axis_size("ep")
    capacity = 3 * top_count * tok_rows // (2 * experts)
    results = layer(
        routing.T,
        gate_weights.T,
        tokens,
        cotangent,
        expert_gate,
        expert_up,
        expert_down,
        n_ep,
        n_tp,
        capacity,
    )
    hidden = expert_gate.shape[2] * n_tp
    gates, ups, downs, token_grad, gate_grad, router_grad, gate_square, up_square, down_square = (
        finish(results, router.T, hidden)
    )
    return (
        token_grad,
        gate_grad.T,
        gates,
        ups,
        downs,
        router_grad,
        gate_square,
        up_square,
        down_square,
    )


def solution(mesh):
    in_specs = (
        P("ep", "tp"),
        P("ep", None),
        P("ep", None),
        P("ep", "tp"),
        P("ep", None, "tp"),
        P("ep", None, "tp"),
        P("ep", "tp", None),
        P(),
    )
    out_specs = (
        P("ep", "tp"),
        P("ep", None),
        P("ep", None, "tp"),
        P("ep", None, "tp"),
        P("ep", "tp", None),
        P("ep", "tp"),
        P("ep", None),
        P("ep", None),
        P("ep", "tp"),
    )
    return jax.shard_map(shards, mesh=mesh, in_specs=in_specs, out_specs=out_specs, check_vma=False)
```
